128 devices in a mesh: sp: 16 (over z, y), tp: 8 (over x, core).
Axes of the slice: x: 4, y: 4, z: 4, core: 2. Of those that a mesh axis runs over, the one named last changes fastest.
Arguments:
- hidden: bfloat16 [16, 1024, 1024], P(None, 'sp'), may hold values from -0.09375 to 0.09375
- value_weight: bfloat16 [1024, 1024], P(None, 'tp'), may hold values from -0.75 to 0.75
- queries: bfloat16 [16, 8, 1024, 64], P(None, 'tp', 'sp'), may hold values from -0.1875 to 0.1875
- key_vectors: bfloat16 [16, 8, 1024, 64], P(None, 'tp', 'sp'), may hold values from -0.1875 to 0.1875
- forward_decay: float32 [16, 8, 1024, 64], P(None, 'tp', 'sp'), may hold values from -0.0029296875 to -9.765625e-06
- backward_decay: float32 [16, 8, 1024, 64], P(None, 'tp', 'sp'), may hold values from -0.0029296875 to -9.765625e-06
- cotangent: bfloat16 [16, 1024, 1024], P(None, 'sp', 'tp'), may hold values from -6 to 6
Outputs:
- grad_queries: bfloat16 [16, 8, 1024, 64], P(None, 'tp', 'sp')
- grad_keys: bfloat16 [16, 8, 1024, 64], P(None, 'tp', 'sp')
- grad_forward: float32 [16, 8, 1024, 64], P(None, 'tp', 'sp')
- grad_backward: float32 [16, 8, 1024, 64], P(None, 'tp', 'sp')
- grad_hidden: bfloat16 [16, 1024, 1024], P(None, 'sp', 'tp')
- grad_weight: float32 [1024, 1024], P('sp', 'tp')
The draws below stay inside these ranges and needn't reach their ends.
All inputs are finite; a program needn't handle non-finite values.
Results may differ from the reference program's by a relative error of at most 0.015.
Values may be sent and summed in bfloat16 or wider, within the bound.
A program may use at most 128 MiB of HBM per device.

```python
import jax
import jax.numpy as jnp
from jax import lax

D = 1024
HEADS = 8
DK = 64
DV = 128
BATCH = 16
TOK_DEV = 64
TOKENS = 1024


def steps_of(rng, shape, cuts, smallest, high):
    level, own = 1.0, jax.random.fold_in(rng, 6)
    for axis_at, parts in cuts:
        heights = jnp.exp(jax.random.uniform(jax.random.fold_in(own, axis_at), (parts,), jnp.float32, smallest / len(cuts), high / len(cuts)))
        level = level * jnp.repeat(heights, shape[axis_at] // parts).reshape([-1 if axis == axis_at else 1 for axis in range(len(shape))])
    return level


def normal_values(key, dims, spread, reach, split=(), kind=jnp.bfloat16):
    values = jax.random.normal(key, dims, jnp.float32) * spread
    if len(split) > 0:
        values = steps_of(key, dims, split, -0.22, 0.18) * values
    return jnp.clip(values, min=-reach, max=reach).astype(kind)


def setup_inputs(seed: int = 0) -> dict:
    keys = jax.random.split(jax.random.key(seed), 8)
    hidden = normal_values(keys[0], (BATCH, TOKENS, D), 0.016, 0.09375, ((1, 16),))
    value_weight = normal_values(keys[1], (D, HEADS * DV), (D // 16) ** -0.5, 0.75, ((1, 8),))
    queries = normal_values(keys[2], (BATCH, HEADS, TOKENS, DK), 0.03, 0.1875, ((1, 8), (2, 16)))
    key_vectors = normal_values(keys[3], (BATCH, HEADS, TOKENS, DK), 0.03, 0.1875, ((1, 8), (2, 16)))
    forward_decay = jnp.clip(-0.0029296875 + 0.002919922 * jax.random.uniform(keys[4], (BATCH, HEADS, TOKENS, DK), jnp.float32) ** steps_of(keys[4], (BATCH, HEADS, TOKENS, DK), ((1, 8), (2, 16)), -0.2, 0.2), -0.0029296875, -9.765624781721272e-06)
    backward_decay = jnp.clip(-0.0029296875 + 0.002919922 * jax.random.uniform(keys[5], (BATCH, HEADS, TOKENS, DK), jnp.float32) ** steps_of(keys[5], (BATCH, HEADS, TOKENS, DK), ((1, 8), (2, 16)), -0.2, 0.2), -0.0029296875, -9.765624781721272e-06)
    cotangent = normal_values(keys[6], (BATCH, TOKENS, HEADS * DV), 1.0, 6.0, ((1, 16), (2, 8)))
    return dict(hidden=hidden, value_weight=value_weight, queries=queries, key_vectors=key_vectors, forward_decay=forward_decay, backward_decay=backward_decay, cotangent=cotangent)


EXACT_DOTS = lax.Precision.HIGHEST


def rounded(tensor):
    return lax.optimization_barrier(tensor.astype(jnp.bfloat16)).astype(jnp.float32)


def elements(query_heads, key_heads, value_heads, decay_heads, seed_heads):
    cumulative = jnp.cumsum(decay_heads, axis=2)
    final_sum = cumulative[:, :, -1, :]
    to_end = jnp.exp(final_sum[:, :, None, :] - cumulative)
    factor = jnp.exp(final_sum)
    state_part = jnp.einsum('bhjd,bhje->bhde', key_heads * to_end, value_heads, precision=EXACT_DOTS)
    grad_part = jnp.einsum('bhcd,bhce->bhde', query_heads * jnp.exp(cumulative), seed_heads, precision=EXACT_DOTS)
    return factor, state_part, grad_part


def block_grads(query_part, key_part, value_part, decay_part, seed_part, state_in, grad_in):
    length = query_part.shape[1]
    value_real = value_part.astype(jnp.float32)
    seed_real = seed_part.astype(jnp.float32)
    cumulative = jnp.cumsum(decay_part, axis=1)
    final_sum = cumulative[:, -1, :]
    growth = jnp.exp(cumulative)
    shrink = jnp.exp(-cumulative)
    to_end = jnp.exp(final_sum[:, None, :] - cumulative)
    query_hat = rounded(query_part * growth)
    key_hat = rounded(key_part * shrink)
    below_mask = jnp.tril(jnp.ones((length, length), dtype=bool))[None]
    scores = rounded(jnp.where(below_mask, jnp.einsum('hid,hjd->hij', query_hat, key_hat, precision=EXACT_DOTS), 0.0))
    seed_scores = rounded(jnp.where(below_mask, jnp.einsum('hie,hje->hij', seed_real, value_real, precision=EXACT_DOTS), 0.0))
    grad_query = growth * (jnp.einsum('hij,hjd->hid', seed_scores, key_hat, precision=EXACT_DOTS)
                           + jnp.einsum('hce,hde->hcd', seed_real, state_in, precision=EXACT_DOTS))
    grad_key = shrink * jnp.einsum('hij,hid->hjd', seed_scores, query_hat, precision=EXACT_DOTS)
    grad_key = grad_key + to_end * jnp.einsum('hde,hje->hjd', grad_in, value_real, precision=EXACT_DOTS)
    grad_value = jnp.einsum('hij,hie->hje', scores, seed_real, precision=EXACT_DOTS)
    grad_value = grad_value + jnp.einsum('hjd,hde->hje', key_part * to_end, grad_in, precision=EXACT_DOTS)
    grad_cumul = query_part * grad_query - key_part * grad_key
    return grad_query, grad_key, grad_value, grad_cumul


def direction(query_seq, key_seq, value_seq, decay_seq, seed_seq):
    head_count, length, key_width = query_seq.shape
    value_width = value_seq.shape[2]
    block_count = length // TOK_DEV

    def to_blocks(tensor):
        return tensor.reshape(head_count, block_count, TOK_DEV, tensor.shape[2]).transpose(1, 0, 2, 3)

    def from_blocks(tensor):
        return tensor.transpose(1, 0, 2, 3).reshape(head_count, length, tensor.shape[3])

    query_blocks, key_blocks = to_blocks(query_seq), to_blocks(key_seq)
    value_blocks, decay_blocks, seed_blocks = to_blocks(value_seq), to_blocks(decay_seq), to_blocks(seed_seq)
    factor, state_part, grad_part = elements(query_blocks, key_blocks, value_blocks.astype(jnp.float32),
                                             decay_blocks, seed_blocks.astype(jnp.float32))

    def advance(carried, pieces):
        return pieces[0][:, :, None] * carried + pieces[1], carried

    zero_state = jnp.zeros((head_count, key_width, value_width), jnp.float32)
    _, state_in = lax.scan(advance, zero_state, (factor, state_part))
    _, grad_in = lax.scan(advance, zero_state, (factor, grad_part), reverse=True)
    results = lax.map(lambda pieces: block_grads(*pieces),
                      (query_blocks, key_blocks, value_blocks, decay_blocks, seed_blocks, state_in, grad_in))
    return tuple(from_blocks(result) for result in results)


def reverse_tokens(tensor):
    return jnp.flip(tensor, axis=1)


def reference(hidden, value_weight, queries, key_vectors, forward_decay, backward_decay, cotangent):
    hidden_rows = hidden.reshape(BATCH * TOKENS, D)
    values_flat = jnp.dot(hidden_rows, value_weight, preferred_element_type=jnp.float32).astype(jnp.bfloat16)
    value_heads = values_flat.reshape(BATCH, TOKENS, HEADS, DV).transpose(0, 2, 1, 3)
    seed_heads = cotangent.reshape(BATCH, TOKENS, HEADS, DV).transpose(0, 2, 1, 3)

    def per_sequence(inputs):
        query_seq, key_seq, value_seq, ahead_decay, behind_decay, seed_seq = inputs
        ahead = direction(query_seq, key_seq, value_seq, ahead_decay, seed_seq)
        behind = direction(reverse_tokens(query_seq), reverse_tokens(key_seq), reverse_tokens(value_seq),
                           reverse_tokens(behind_decay), reverse_tokens(seed_seq))
        cumul_ahead = ahead[3]
        cumul_behind = reverse_tokens(behind[3])
        grad_ahead = -(jnp.cumsum(cumul_ahead, axis=1) - cumul_ahead)
        grad_behind = jnp.cumsum(cumul_behind, axis=1)
        return (ahead[0] + reverse_tokens(behind[0]), ahead[1] + reverse_tokens(behind[1]),
                ahead[2] + reverse_tokens(behind[2]), grad_ahead, grad_behind)

    grad_query, grad_key, grad_value, grad_ahead, grad_behind = lax.map(
        per_sequence, (queries.astype(jnp.float32), key_vectors.astype(jnp.float32), value_heads,
                       forward_decay, backward_decay, seed_heads))
    value_rows = grad_value.transpose(0, 2, 1, 3).reshape(BATCH * TOKENS, HEADS * DV).astype(jnp.bfloat16)
    grad_hidden = lax.dot_general(value_rows, value_weight, (((1,), (1,)), ((), ())),
                                  preferred_element_type=jnp.float32).astype(jnp.bfloat16).reshape(BATCH, TOKENS, D)
    grad_weight = lax.dot_general(hidden_rows, value_rows, (((0,), (0,)), ((), ())),
                                  preferred_element_type=jnp.float32)
    return (grad_query.astype(jnp.bfloat16), grad_key.astype(jnp.bfloat16), grad_ahead, grad_behind,
            grad_hidden, grad_weight)
```

```python
import functools

import jax
import jax.numpy as jnp
from jax import lax
from jax.experimental import pallas as pl
from jax.experimental.pallas import tpu as pltpu
from jax.sharding import PartitionSpec as P

MESH = pl.DeviceIdType.MESH
F32, BF16 = jnp.float32, jnp.bfloat16
SP, TP = 16, 8
BATCH, TOK, DK, DV, WIDTH = 16, 64, 64, 128, 1024
ROWS = BATCH * TOK
BLK = 256
NBLK = ROWS // BLK
STEP = 2.0**-16
QK, DEC, DO, VV, DVT, DQK, GG, GW = range(8)


def iota(shape, axis):
    return lax.broadcasted_iota(jnp.int32, shape, axis)


def dot(a, b):
    return lax.dot_general(a, b, (((1,), (0,)), ((), ())), preferred_element_type=F32)


def dot_nt(a, b):
    return lax.dot_general(a, b, (((1,), (1,)), ((), ())), preferred_element_type=F32)


def dot_tn(a, b):
    return lax.dot_general(a, b, (((0,), (0,)), ((), ())), preferred_element_type=F32)


def hi_lo(x):
    hi = x.astype(BF16)
    lo = (x - hi.astype(F32)).astype(BF16)
    return jnp.concatenate([hi, lo], axis=1)


def tri(group):
    r, c = iota((BLK, BLK), 0), iota((BLK, BLK), 1)
    keep = r >= c
    if group < BLK:
        keep = keep & (r // group == c // group)
    return jnp.where(keep, 1.0, 0.0).astype(BF16)


def tile(ref, index):
    return ref.at[pl.ds(pl.multiple_of(index * TOK, TOK), TOK)]


def kernel(
    hidden,
    weight,
    q_hbm,
    k_hbm,
    df_hbm,
    db_hbm,
    cot,
    dq_out,
    dk_out,
    gf_out,
    gb_out,
    gh_out,
    gw_out,
    hid,
    w,
    q_in,
    k_in,
    df_in,
    db_in,
    sends,
    recvs,
    qhat,
    khat,
    grow,
    gsum,
    gcum,
    parts,
    dall,
    wx,
    acc,
    hid_t,
    in_sem,
    ss,
    rs,
    loc_sem,
    wss,
    wrs,
    xss,
    xrs,
    pss,
    prs,
):
    me = lax.axis_index("sp")
    tp = lax.axis_index("tp")
    y, z = me % 4, me // 4
    core, xc = tp % 2, tp // 2

    loads = [
        pltpu.make_async_copy(q_hbm, q_in, in_sem.at[0]),
        pltpu.make_async_copy(k_hbm, k_in, in_sem.at[1]),
        pltpu.make_async_copy(df_hbm, df_in, in_sem.at[2]),
        pltpu.make_async_copy(db_hbm, db_in, in_sem.at[3]),
        pltpu.make_async_copy(cot, sends.at[DO], in_sem.at[4]),
        pltpu.make_async_copy(weight, w, in_sem.at[5]),
        pltpu.make_async_copy(hidden, hid, in_sem.at[6]),
    ]
    for load in loads:
        load.start()

    barrier = pltpu.get_barrier_semaphore()

    def greet_sp(r, carry):
        pl.semaphore_signal(
            barrier, inc=1, device_id={"sp": (me + r) % SP}, device_id_type=MESH
        )
        return carry

    def greet_tp(r, carry):
        pl.semaphore_signal(
            barrier, inc=1, device_id={"tp": (tp + r) % TP}, device_id_type=MESH
        )
        return carry

    lax.fori_loop(1, SP, greet_sp, 0)
    lax.fori_loop(1, TP, greet_tp, 0)

    def peer_of(r):
        m = (r * 7) % SP
        return ((z + m // 4) % 4) * 4 + (y + m % 4) % 4

    def sp_copy(kind, r):
        to = peer_of(r)
        src = tile(sends.at[kind], to)
        if kind == DVT:
            dst = dall.at[pl.ds(pl.multiple_of(tp * ROWS + me * TOK, TOK), TOK)]
        else:
            dst = tile(recvs.at[kind], me)
        return pltpu.make_async_remote_copy(
            src_ref=src,
            dst_ref=dst,
            send_sem=ss.at[kind, r],
            recv_sem=rs.at[kind, me],
            device_id={"sp": to},
            device_id_type=MESH,
        )

    def sp_arrived(kind, r):
        frm = peer_of(r)
        if kind == DVT:
            dst = dall.at[pl.ds(pl.multiple_of(tp * ROWS + frm * TOK, TOK), TOK)]
        else:
            dst = tile(recvs.at[kind], frm)
        pltpu.make_async_remote_copy(
            src_ref=dst,
            dst_ref=dst,
            send_sem=ss.at[kind, r],
            recv_sem=rs.at[kind, frm],
            device_id={"sp": frm},
            device_id_type=MESH,
        ).wait_recv()

    def own_copy(kind):
        if kind == DVT:
            dst = dall.at[pl.ds(pl.multiple_of(tp * ROWS + me * TOK, TOK), TOK)]
        else:
            dst = tile(recvs.at[kind], me)
        return pltpu.make_async_copy(tile(sends.at[kind], me), dst, loc_sem.at[kind])

    def send_all(kind):
        def body(r, carry):
            sp_copy(kind, r).start()
            return carry

        lax.fori_loop(1, SP, body, 0)
        own_copy(kind).start()

    def wait_all(kind):
        def body(r, carry):
            sp_arrived(kind, r)
            return carry

        lax.fori_loop(1, SP, body, 0)
        own_copy(kind).wait()

    loads[0].wait()
    loads[1].wait()
    sends[QK] = jnp.concatenate(
        [q_in[...].reshape(ROWS, DK), k_in[...].reshape(ROWS, DK)], axis=1
    )
    loads[2].wait()
    loads[3].wait()
    low = tri(TOK)
    for b in range(NBLK):
        span = pl.ds(b * 4, 4)
        both = jnp.concatenate(
            [df_in[span].reshape(BLK, DK), db_in[span].reshape(BLK, DK)], axis=1
        )
        run = dot(low, hi_lo(both))
        steps = jnp.round((run[:, :DV] + run[:, DV:]) * (1.0 / STEP))
        before = jnp.where(iota((BLK, DV), 0) % TOK == 0, 0.0, pltpu.roll(steps, 1, 0))
        sends[DEC, pl.ds(b * BLK, BLK)] = ((steps - before) * STEP).astype(BF16)
    loads[4].wait()
    loads[5].wait()
    pl.semaphore_wait(barrier, SP + TP - 2)
    send_all(DEC)
    send_all(QK)
    send_all(DO)

    def w_copy(r):
        to = (tp + r) % TP
        return pltpu.make_async_remote_copy(
            src_ref=w.at[pl.ds(pl.multiple_of(to * DV, DV), DV)],
            dst_ref=wx.at[pl.ds(pl.multiple_of(tp * DV, DV), DV)],
            send_sem=wss.at[r],
            recv_sem=wrs.at[r],
            device_id={"tp": to},
            device_id_type=MESH,
        )

    def w_send(r, carry):
        w_copy(r).start()
        return carry

    lax.fori_loop(1, TP, w_send, 0)
    own_w = pltpu.make_async_copy(
        w.at[pl.ds(pl.multiple_of(tp * DV, DV), DV)],
        wx.at[pl.ds(pl.multiple_of(tp * DV, DV), DV)],
        wrs.at[0],
    )
    own_w.start()

    loads[6].wait()
    for b in range(NBLK):
        rows = hid[pl.ds(b * 4, 4)].reshape(BLK, WIDTH)
        sends[VV, pl.ds(b * BLK, BLK)] = dot(rows, w[...]).astype(BF16)
    send_all(VV)

    def turn(t, carry):
        at = pl.ds(pl.multiple_of(t * 128, 128), 128)
        hid_t[:, at] = hid[pl.ds(t * 2, 2)].reshape(128, WIDTH).T
        return carry

    lax.fori_loop(0, ROWS // 128, turn, 0)

    wait_all(DEC)
    lane_f = iota((BLK, DV), 1) < DK
    full = tri(BLK)
    base = jnp.zeros((1, DV), F32)
    cums = []
    for b in range(NBLK):
        d = recvs[DEC, pl.ds(b * BLK, BLK)]
        inside = dot(full, d) + base
        base = inside[BLK - 1 :, :]
        cums.append(jnp.where(lane_f, inside, d.astype(F32) - inside))
    wait_all(QK)
    for b in range(NBLK):
        at = pl.ds(b * BLK, BLK)
        growth = jnp.exp(cums[b])
        shrink = jnp.exp(-cums[b])
        qk = recvs[QK, at].astype(F32)
        kq = pltpu.roll(qk, DK, 1)
        qhat[at] = (jnp.where(lane_f, qk, kq) * growth).astype(BF16)
        khat[at] = (jnp.where(lane_f, kq, qk) * shrink).astype(BF16)
        grow[at] = growth
    wait_all(DO)
    row_f = iota((DV, DV), 0) < DK

    def others(pieces):
        result = []
        zero = jnp.zeros((DV, DV), F32)
        after = [zero] * NBLK
        before = [zero] * NBLK
        for b in range(NBLK - 2, -1, -1):
            after[b] = after[b + 1] + pieces[b + 1]
        for b in range(1, NBLK):
            before[b] = before[b - 1] + pieces[b - 1]
        return after, before

    pieces = [
        dot_tn(qhat[pl.ds(b * BLK, BLK)], recvs[DO, pl.ds(b * BLK, BLK)]) for b in range(NBLK)
    ]
    after, before = others(pieces)
    for b in range(NBLK):
        parts[0, pl.ds(b * DV, DV)] = jnp.where(row_f, after[b], before[b]).astype(BF16)

    r_, c_ = iota((BLK, BLK), 0), iota((BLK, BLK), 1)
    zero16 = jnp.zeros((), BF16)
    for jj in range(NBLK):
        blk = (z + jj) % NBLK
        at = pl.ds(pl.multiple_of(blk * BLK, BLK), BLK)
        pat = pl.ds(pl.multiple_of(blk * DV, DV), DV)
        qh, kh, do = qhat[at], khat[at], recvs[DO, at]
        fwd = dot_nt(jnp.where(lane_f, kh, zero16), qh)
        bwd = dot_nt(jnp.where(lane_f, zero16, kh), qh)
        scores = jnp.where(r_ <= c_, fwd, 0.0) + jnp.where(r_ >= c_, bwd, 0.0)
        dv = dot(kh, parts[0, pat]) + dot(scores.astype(BF16), do)
        sends[DVT, at] = dv.astype(BF16)
        for i in range(4):
            a = (y + i) % 4

            def go(a=a, jj=jj, blk=blk):
                to = blk * 4 + a
                pltpu.make_async_remote_copy(
                    src_ref=tile(sends.at[DVT], to),
                    dst_ref=dall.at[pl.ds(pl.multiple_of(tp * ROWS + me * TOK, TOK), TOK)],
                    send_sem=ss.at[DVT, jj * 4 + i],
                    recv_sem=rs.at[DVT, me],
                    device_id={"sp": to},
                    device_id_type=MESH,
                ).start()

            if jj == 0 and i == 0:
                own_copy(DVT).start()
            else:
                go()

    wait_all(VV)
    pieces = [
        dot_tn(khat[pl.ds(b * BLK, BLK)], recvs[VV, pl.ds(b * BLK, BLK)]) for b in range(NBLK)
    ]
    after, before = others(pieces)
    for b in range(NBLK):
        parts[1, pl.ds(b * DV, DV)] = jnp.where(row_f, before[b], after[b]).astype(BF16)
    base = jnp.zeros((1, DV), F32)
    for b in range(NBLK):
        at = pl.ds(b * BLK, BLK)
        pat = pl.ds(b * DV, DV)
        qh, kh, do, v = qhat[at], khat[at], recvs[DO, at], recvs[VV, at]
        growth = grow[at]
        s = dot_nt(do, v).astype(BF16)
        st = dot_nt(v, do).astype(BF16)
        x = dot_nt(do, parts[1, pat])
        x = x + dot(jnp.where(r_ >= c_, s, zero16), jnp.where(lane_f, kh, zero16))
        x = x + dot(jnp.where(r_ <= c_, s, zero16), jnp.where(lane_f, zero16, kh))
        yk = dot_nt(v, parts[0, pat])
        yk = yk + dot(jnp.where(r_ <= c_, st, zero16), jnp.where(lane_f, qh, zero16))
        yk = yk + dot(jnp.where(r_ >= c_, st, zero16), jnp.where(lane_f, zero16, qh))
        g = qh.astype(F32) * x - kh.astype(F32) * yk
        run = dot(full, hi_lo(g))
        run = run[:, :DV] + run[:, DV:] + base
        base = run[BLK - 1 :, :]
        sends[GG, at] = jnp.where(lane_f, g - run, run).astype(BF16)
        dq2 = x * growth
        dk2 = yk / growth
        dq2 = dq2 + pltpu.roll(dq2, DK, 1)
        dk2 = dk2 + pltpu.roll(dk2, DK, 1)
        sends[DQK, at] = jnp.where(lane_f, dq2, dk2).astype(BF16)
    send_all(DQK)
    send_all(GG)

    wait_all(DVT)
    chip = ((xc + 1) % 4, (xc + 3) % 4, (xc + 2) % 4)

    def head(index):
        return dall.at[pl.ds(pl.multiple_of(index * ROWS, ROWS), ROWS)]

    def x_copy(i):
        return pltpu.make_async_remote_copy(
            src_ref=head(tp),
            dst_ref=head(tp),
            send_sem=xss.at[i],
            recv_sem=xrs.at[i],
            device_id={"tp": chip[i] * 2 + core},
            device_id_type=MESH,
        )

    def x_arrived(i):
        frm = (chip[1], chip[0], chip[2])[i]
        spot = head(frm * 2 + core)
        pltpu.make_async_remote_copy(
            src_ref=spot,
            dst_ref=spot,
            send_sem=xss.at[i],
            recv_sem=xrs.at[i],
            device_id={"tp": frm * 2 + core},
            device_id_type=MESH,
        ).wait_recv()
        return frm

    def p_copy(i, index):
        return pltpu.make_async_remote_copy(
            src_ref=head(index),
            dst_ref=head(index),
            send_sem=pss.at[i],
            recv_sem=prs.at[i],
            device_id={"tp": xc * 2 + 1 - core},
            device_id_type=MESH,
        )

    for i in range(3):
        x_copy(i).start()
    p_copy(3, tp).start()
    drows = dall[pl.ds(pl.multiple_of(tp * ROWS, ROWS), ROWS)]
    for b in range(NBLK):
        at = pl.ds(b * BLK, BLK)
        sends[GW, at] = dot(hid_t[at], drows).astype(BF16)
    send_all(GW)

    wait_all(DQK)
    for b in range(NBLK):
        at = pl.ds(b * BLK, BLK)
        both = recvs[DQK, at]
        dq_out[pl.ds(b * 4, 4)] = both[:, :DK].reshape(4, TOK, DK)
        dk_out[pl.ds(b * 4, 4)] = both[:, DK:].reshape(4, TOK, DK)
    wait_all(GG)
    for b in range(NBLK):
        at = pl.ds(b * BLK, BLK)
        both = recvs[GG, at].astype(F32)
        gf_out[pl.ds(b * 4, 4)] = both[:, :DK].reshape(4, TOK, DK)
        gb_out[pl.ds(b * 4, 4)] = both[:, DK:].reshape(4, TOK, DK)

    def w_arrived(r, carry):
        frm = (tp + TP - r) % TP
        spot = wx.at[pl.ds(pl.multiple_of(frm * DV, DV), DV)]
        pltpu.make_async_remote_copy(
            src_ref=spot,
            dst_ref=spot,
            send_sem=wss.at[r],
            recv_sem=wrs.at[r],
            device_id={"tp": frm},
            device_id_type=MESH,
        ).wait_recv()
        return carry

    lax.fori_loop(1, TP, w_arrived, 0)
    own_w.wait()

    def term(index):
        rows = dall[pl.ds(pl.multiple_of(index * ROWS, ROWS), ROWS)]
        return dot_nt(rows, wx[pl.ds(pl.multiple_of(index * DV, DV), DV)])

    other = xc * 2 + 1 - core
    p_copy(3, other).wait_recv()
    acc[...] = term(tp) + term(other)
    for i in range(3):
        frm = x_arrived(i)
        p_copy(i, frm * 2 + core).start()
        acc[...] += term(frm * 2 + core)
        p_copy(i, frm * 2 + 1 - core).wait_recv()
        if i < 2:
            acc[...] += term(frm * 2 + 1 - core)
        else:
            gh_out[...] = (acc[...] + term(frm * 2 + 1 - core)).astype(BF16).reshape(BATCH, TOK, DV)

    wait_all(GW)
    total = jnp.zeros((TOK, DV), F32)
    for b in range(SP):
        total = total + recvs[GW, pl.ds(b * TOK, TOK)].astype(F32)
    gw_out[...] = total

    def left(r, carry):
        for kind in range(8):
            sp_copy(kind, r).wait_send()
        return carry

    lax.fori_loop(1, SP, left, 0)

    def w_left(r, carry):
        w_copy(r).wait_send()
        return carry

    lax.fori_loop(1, TP, w_left, 0)
    for i in range(3):
        x_copy(i).wait_send()
        p_copy(i, tp).wait_send()
    p_copy(3, tp).wait_send()


def per_device(hidden, value_weight, queries, key_vectors, forward_decay, backward_decay, cotangent):
    any_space = pl.BlockSpec(memory_space=pl.ANY)
    vmem = pl.BlockSpec(memory_space=pltpu.VMEM)
    narrow = (BATCH, TOK, DK)
    sem = pltpu.SemaphoreType.DMA
    outs = pl.pallas_call(
        kernel,
        out_shape=(
            jax.ShapeDtypeStruct(narrow, BF16),
            jax.ShapeDtypeStruct(narrow, BF16),
            jax.ShapeDtypeStruct(narrow, F32),
            jax.ShapeDtypeStruct(narrow, F32),
            jax.ShapeDtypeStruct((BATCH, TOK, DV), BF16),
            jax.ShapeDtypeStruct((WIDTH // SP, DV), F32),
        ),
        in_specs=[any_space] * 7,
        out_specs=(vmem,) * 6,
        scratch_shapes=[
            pltpu.VMEM((BATCH, TOK, WIDTH), BF16),
            pltpu.VMEM((WIDTH, DV), BF16),
            pltpu.VMEM(narrow, BF16),
            pltpu.VMEM(narrow, BF16),
            pltpu.VMEM(narrow, F32),
            pltpu.VMEM(narrow, F32),
            pltpu.VMEM((8, ROWS, DV), BF16),
            pltpu.VMEM((8, ROWS, DV), BF16),
            pltpu.VMEM((ROWS, DV), BF16),
            pltpu.VMEM((ROWS, DV), BF16),
            pltpu.VMEM((ROWS, DV), F32),
            pltpu.VMEM((8, DV), F32),
            pltpu.VMEM((8, DV), F32),
            pltpu.VMEM((2, NBLK * DV, DV), BF16),
            pltpu.VMEM((TP * ROWS, DV), BF16),
            pltpu.VMEM((TP * DV, DV), BF16),
            pltpu.VMEM((ROWS, DV), F32),
            pltpu.VMEM((WIDTH, ROWS), BF16),
            sem((7,)),
            sem((8, SP)),
            sem((8, SP)),
            sem((8,)),
            sem((TP,)),
            sem((TP,)),
            sem((3,)),
            sem((3,)),
            sem((4,)),
            sem((4,)),
        ],
        compiler_params=pltpu.CompilerParams(
            collective_id=0, has_side_effects=True, vmem_limit_bytes=60 << 20
        ),
    )(
        hidden,
        value_weight,
        queries.reshape(narrow),
        key_vectors.reshape(narrow),
        forward_decay.reshape(narrow),
        backward_decay.reshape(narrow),
        cotangent.reshape(ROWS, DV),
    )
    heads = (BATCH, 1, TOK, DK)
    return tuple(out.reshape(heads) for out in outs[:4]) + tuple(outs[4:])


def solution(mesh):
    spread = P(None, "tp", "sp", None)
    return jax.shard_map(
        per_device,
        mesh=mesh,
        in_specs=(
            P(None, "sp", None),
            P(None, "tp"),
            spread,
            spread,
            spread,
            spread,
            P(None, "sp", "tp"),
        ),
        out_specs=(spread, spread, spread, spread, P(None, "sp", "tp"), P("sp", "tp")),
        check_vma=False,
    )
```

```python
import functools

import jax
import jax.numpy as jnp
from jax import lax
from jax.experimental import pallas as pl
from jax.experimental.pallas import tpu as pltpu
from jax.sharding import PartitionSpec as P

MESH = pl.DeviceIdType.MESH
F32, BF16 = jnp.float32, jnp.bfloat16
SP, TP = 16, 8
BATCH, TOK, DK, DV, WIDTH = 16, 64, 64, 128, 1024
ROWS = BATCH * TOK
BLK = 256
NBLK = ROWS // BLK
STEP = 2.0**-16
QK, DEC, DO, VV, DVT, DQK, GG, GW = range(8)


def iota(shape, axis):
    return lax.broadcasted_iota(jnp.int32, shape, axis)


def dot(a, b):
    return lax.dot_general(a, b, (((1,), (0,)), ((), ())), preferred_element_type=F32)


def dot_nt(a, b):
    return lax.dot_general(a, b, (((1,), (1,)), ((), ())), preferred_element_type=F32)


def dot_tn(a, b):
    return lax.dot_general(a, b, (((0,), (0,)), ((), ())), preferred_element_type=F32)


def hi_lo(x):
    hi = x.astype(BF16)
    lo = (x - hi.astype(F32)).astype(BF16)
    return jnp.concatenate([hi, lo], axis=1)


def tri(group):
    r, c = iota((BLK, BLK), 0), iota((BLK, BLK), 1)
    keep = r >= c
    if group < BLK:
        keep = keep & (r // group == c // group)
    return jnp.where(keep, 1.0, 0.0).astype(BF16)


def tile(ref, index):
    return ref.at[pl.ds(pl.multiple_of(index * TOK, TOK), TOK)]


def kernel(
    hidden,
    weight,
    q_hbm,
    k_hbm,
    df_hbm,
    db_hbm,
    cot,
    dqk_out,
    gg_out,
    gh_out,
    gw_out,
    hid,
    w,
    q_in,
    k_in,
    df_in,
    db_in,
    sends,
    recvs,
    qhat,
    khat,
    grow,
    gterm,
    scores,
    parts,
    dall,
    wx,
    acc,
    hid_t,
    in_sem,
    ss,
    rs,
    loc_sem,
    wss,
    wrs,
    xss,
    xrs,
    pss,
    prs,
):
    me = lax.axis_index("sp")
    tp = lax.axis_index("tp")
    y, z = me % 4, me // 4
    core, xc = tp % 2, tp // 2
    barrier = pltpu.get_barrier_semaphore()

    def greet_sp(r, carry):
        pl.semaphore_signal(
            barrier, inc=1, device_id={"sp": (me + r) % SP}, device_id_type=MESH
        )
        return carry

    def greet_tp(r, carry):
        pl.semaphore_signal(
            barrier, inc=1, device_id={"tp": (tp + r) % TP}, device_id_type=MESH
        )
        return carry

    lax.fori_loop(1, SP, greet_sp, 0)
    lax.fori_loop(1, TP, greet_tp, 0)

    loads = [
        pltpu.make_async_copy(df_hbm, df_in, in_sem.at[2]),
        pltpu.make_async_copy(db_hbm, db_in, in_sem.at[3]),
        pltpu.make_async_copy(q_hbm, q_in, in_sem.at[0]),
        pltpu.make_async_copy(k_hbm, k_in, in_sem.at[1]),
        pltpu.make_async_copy(cot, sends.at[DO], in_sem.at[4]),
        pltpu.make_async_copy(weight, w, in_sem.at[5]),
        pltpu.make_async_copy(hidden, hid, in_sem.at[6]),
    ]
    for load in loads:
        load.start()

    def peer_of(r):
        m = (r * 7) % SP
        return ((z + m // 4) % 4) * 4 + (y + m % 4) % 4

    def landing(kind, frm):
        if kind == DVT:
            return dall.at[pl.ds(pl.multiple_of(tp * ROWS + frm * TOK, TOK), TOK)]
        return tile(recvs.at[kind], frm)

    def sp_copy(kind, r, to):
        return pltpu.make_async_remote_copy(
            src_ref=tile(sends.at[kind], to),
            dst_ref=landing(kind, me),
            send_sem=ss.at[kind, r],
            recv_sem=rs.at[kind, me],
            device_id={"sp": to},
            device_id_type=MESH,
        )

    def sp_wait(kind, r, frm):
        pltpu.make_async_remote_copy(
            src_ref=landing(kind, frm),
            dst_ref=landing(kind, frm),
            send_sem=ss.at[kind, r],
            recv_sem=rs.at[kind, frm],
            device_id={"sp": frm},
            device_id_type=MESH,
        ).wait_recv()

    def own_copy(kind):
        return pltpu.make_async_copy(
            tile(sends.at[kind], me), landing(kind, me), loc_sem.at[kind]
        )

    def send_all(kind):
        def body(r, carry):
            sp_copy(kind, r, peer_of(r)).start()
            return carry

        lax.fori_loop(1, SP, body, 0)
        own_copy(kind).start()

    def wait_all(kind):
        def body(r, carry):
            sp_wait(kind, r, peer_of(r))
            return carry

        lax.fori_loop(1, SP, body, 0)
        own_copy(kind).wait()

    def send_block(kind, jj, blk):
        for i in range(4):
            if jj == 0 and i == 0:
                own_copy(kind).start()
            else:
                sp_copy(kind, jj * 4 + i, blk * 4 + (y + i) % 4).start()

    def wait_plane(kind, jj, plane):
        for i in range(4):
            if jj == 0 and i == 0:
                own_copy(kind).wait()
            else:
                sp_wait(kind, jj * 4 + i, plane * 4 + (y + i) % 4)

    loads[0].wait()
    loads[1].wait()
    low = tri(TOK)
    for b in range(NBLK):
        span = pl.ds(b * 4, 4)
        both = jnp.concatenate(
            [df_in[span].reshape(BLK, DK), db_in[span].reshape(BLK, DK)], axis=1
        )
        run = dot(low, hi_lo(both))
        steps = jnp.round((run[:, :DV] + run[:, DV:]) * (1.0 / STEP))
        before = jnp.where(iota((BLK, DV), 0) % TOK == 0, 0.0, pltpu.roll(steps, 1, 0))
        sends[DEC, pl.ds(b * BLK, BLK)] = ((steps - before) * STEP).astype(BF16)
    loads[2].wait()
    loads[3].wait()
    sends[QK] = jnp.concatenate(
        [q_in[...].reshape(ROWS, DK), k_in[...].reshape(ROWS, DK)], axis=1
    )
    loads[4].wait()
    loads[5].wait()
    pl.semaphore_wait(barrier, SP + TP - 2)
    send_all(DEC)
    send_all(QK)
    send_all(DO)

    def w_copy(r):
        to = (tp + r) % TP
        return pltpu.make_async_remote_copy(
            src_ref=w.at[pl.ds(pl.multiple_of(to * DV, DV), DV)],
            dst_ref=wx.at[pl.ds(pl.multiple_of(tp * DV, DV), DV)],
            send_sem=wss.at[r],
            recv_sem=wrs.at[r],
            device_id={"tp": to},
            device_id_type=MESH,
        )

    def w_send(r, carry):
        w_copy(r).start()
        return carry

    lax.fori_loop(1, TP, w_send, 0)
    own_w = pltpu.make_async_copy(
        w.at[pl.ds(pl.multiple_of(tp * DV, DV), DV)],
        wx.at[pl.ds(pl.multiple_of(tp * DV, DV), DV)],
        wrs.at[0],
    )
    own_w.start()

    loads[6].wait()
    for b in range(NBLK):
        rows = hid[pl.ds(b * 4, 4)].reshape(BLK, WIDTH)
        sends[VV, pl.ds(b * BLK, BLK)] = dot(rows, w[...]).astype(BF16)
    send_all(VV)

    def turn(t, carry):
        at = pl.ds(pl.multiple_of(t * 128, 128), 128)
        hid_t[:, at] = hid[pl.ds(t * 2, 2)].reshape(128, WIDTH).T
        return carry

    lax.fori_loop(0, ROWS // 128, turn, 0)

    wait_all(DEC)
    lane_f = iota((BLK, DV), 1) < DK
    full = tri(BLK)
    base = jnp.zeros((1, DV), F32)
    cums = []
    for b in range(NBLK):
        d = recvs[DEC, pl.ds(b * BLK, BLK)]
        inside = dot(full, d) + base
        base = inside[BLK - 1 :, :]
        cums.append(jnp.where(lane_f, inside, d.astype(F32) - inside))
    wait_all(QK)
    r_, c_ = iota((BLK, BLK), 0), iota((BLK, BLK), 1)
    zero16 = jnp.zeros((), BF16)
    for b in range(NBLK):
        at = pl.ds(b * BLK, BLK)
        growth = jnp.exp(cums[b])
        shrink = jnp.exp(-cums[b])
        qk = recvs[QK, at].astype(F32)
        kq = pltpu.roll(qk, DK, 1)
        qh = (jnp.where(lane_f, qk, kq) * growth).astype(BF16)
        kh = (jnp.where(lane_f, kq, qk) * shrink).astype(BF16)
        qhat[at] = qh
        khat[at] = kh
        grow[at] = growth
        fwd = dot_nt(jnp.where(lane_f, kh, zero16), qh)
        bwd = dot_nt(jnp.where(lane_f, zero16, kh), qh)
        both = jnp.where(r_ <= c_, fwd, 0.0) + jnp.where(r_ >= c_, bwd, 0.0)
        scores[at] = both.astype(BF16)
    row_f = iota((DV, DV), 0) < DK

    def others(pieces):
        zero = jnp.zeros((DV, DV), F32)
        after, before = [zero] * NBLK, [zero] * NBLK
        for b in range(NBLK - 2, -1, -1):
            after[b] = after[b + 1] + pieces[b + 1]
        for b in range(1, NBLK):
            before[b] = before[b - 1] + pieces[b - 1]
        return after, before

    wait_all(DO)
    pieces = [
        dot_tn(qhat[pl.ds(b * BLK, BLK)], recvs[DO, pl.ds(b * BLK, BLK)]) for b in range(NBLK)
    ]
    after, before = others(pieces)
    for b in range(NBLK):
        parts[0, pl.ds(b * DV, DV)] = jnp.where(row_f, after[b], before[b]).astype(BF16)
    for jj in range(NBLK):
        blk = (z + jj) % NBLK
        at = pl.ds(pl.multiple_of(blk * BLK, BLK), BLK)
        pat = pl.ds(pl.multiple_of(blk * DV, DV), DV)
        dv = dot(khat[at], parts[0, pat]) + dot(scores[at], recvs[DO, at])
        sends[DVT, at] = dv.astype(BF16)
        send_block(DVT, jj, blk)

    right, left, far = (xc + 1) % 4, (xc + 3) % 4, (xc + 2) % 4

    def piece(head, cc):
        row = head * ROWS + ((z + 4 - cc) % 4) * BLK
        return dall.at[pl.ds(pl.multiple_of(row, BLK), BLK)]

    def hop(head, cc, sems_s, sems_r, slot, to):
        return pltpu.make_async_remote_copy(
            src_ref=piece(head, cc),
            dst_ref=piece(head, cc),
            send_sem=sems_s.at[slot, cc],
            recv_sem=sems_r.at[slot, cc],
            device_id={"tp": to},
            device_id_type=MESH,
        )

    def to_chip(head, cc, slot, chip):
        return hop(head, cc, xss, xrs, slot, chip * 2 + core)

    def to_core(head, cc, slot):
        return hop(head, cc, pss, prs, slot, xc * 2 + 1 - core)

    def first_hops(cc):
        wait_plane(DVT, cc, (z + 4 - cc) % 4)
        to_chip(tp, cc, 0, right).start()
        to_chip(tp, cc, 1, left).start()
        to_core(tp, cc, 0).start()

    wait_all(VV)
    pieces = [
        dot_tn(khat[pl.ds(b * BLK, BLK)], recvs[VV, pl.ds(b * BLK, BLK)]) for b in range(NBLK)
    ]
    after, before = others(pieces)
    for b in range(NBLK):
        parts[1, pl.ds(b * DV, DV)] = jnp.where(row_f, before[b], after[b]).astype(BF16)
    for jj in range(NBLK):
        blk = (z + jj) % NBLK
        at = pl.ds(pl.multiple_of(blk * BLK, BLK), BLK)
        pat = pl.ds(pl.multiple_of(blk * DV, DV), DV)
        qh, kh, do, v = qhat[at], khat[at], recvs[DO, at], recvs[VV, at]
        growth = grow[at]
        s = dot_nt(do, v).astype(BF16)
        st = dot_nt(v, do).astype(BF16)
        x = dot_nt(do, parts[1, pat])
        x = x + dot(jnp.where(r_ >= c_, s, zero16), jnp.where(lane_f, kh, zero16))
        x = x + dot(jnp.where(r_ <= c_, s, zero16), jnp.where(lane_f, zero16, kh))
        yk = dot_nt(v, parts[0, pat])
        yk = yk + dot(jnp.where(r_ <= c_, st, zero16), jnp.where(lane_f, qh, zero16))
        yk = yk + dot(jnp.where(r_ >= c_, st, zero16), jnp.where(lane_f, zero16, qh))
        gterm[at] = qh.astype(F32) * x - kh.astype(F32) * yk
        dq2 = x * growth
        dk2 = yk / growth
        dq2 = dq2 + pltpu.roll(dq2, DK, 1)
        dk2 = dk2 + pltpu.roll(dk2, DK, 1)
        sends[DQK, at] = jnp.where(lane_f, dq2, dk2).astype(BF16)
        send_block(DQK, jj, blk)
        first_hops(jj)
    base = jnp.zeros((1, DV), F32)
    for b in range(NBLK):
        at = pl.ds(b * BLK, BLK)
        g = gterm[at]
        run = dot(full, hi_lo(g))
        run = run[:, :DV] + run[:, DV:] + base
        base = run[BLK - 1 :, :]
        sends[GG, at] = jnp.where(lane_f, g - run, run).astype(BF16)

    drows = dall[pl.ds(pl.multiple_of(tp * ROWS, ROWS), ROWS)]
    for b in range(NBLK):
        at = pl.ds(b * BLK, BLK)
        sends[GW, at] = dot(hid_t[at], drows).astype(BF16)
    send_all(GW)
    send_all(GG)

    def w_arrived(r, carry):
        frm = (tp + TP - r) % TP
        spot = wx.at[pl.ds(pl.multiple_of(frm * DV, DV), DV)]
        pltpu.make_async_remote_copy(
            src_ref=spot,
            dst_ref=spot,
            send_sem=wss.at[r],
            recv_sem=wrs.at[r],
            device_id={"tp": frm},
            device_id_type=MESH,
        ).wait_recv()
        return carry

    lax.fori_loop(1, TP, w_arrived, 0)
    own_w.wait()

    def term(chip, cc):
        total = None
        for c in range(2):
            head = chip * 2 + c
            row = head * ROWS + ((z + 4 - cc) % 4) * BLK
            rows = dall[pl.ds(pl.multiple_of(row, BLK), BLK)]
            part = dot_nt(rows, wx[pl.ds(pl.multiple_of(head * DV, DV), DV)])
            total = part if total is None else total + part
        return total

    for cc in range(4):
        head_l, head_r = left * 2 + core, right * 2 + core
        to_chip(head_l, cc, 0, left).wait_recv()
        if cc % 2 == 0:
            to_chip(head_l, cc, 2, right).start()
        to_core(head_l, cc, 1).start()
        to_chip(head_r, cc, 1, right).wait_recv()
        if cc % 2 == 1:
            to_chip(head_r, cc, 2, left).start()
        to_core(head_r, cc, 2).start()
    for cc in range(4):
        for slot, chip in ((0, xc), (1, left), (2, right)):
            to_core(chip * 2 + 1 - core, cc, slot).wait_recv()
        acc[pl.ds(cc * BLK, BLK)] = term(xc, cc) + term(left, cc) + term(right, cc)
    for cc in range(4):
        to_chip(far * 2 + core, cc, 2, far).wait_recv()
        to_core(far * 2 + core, cc, 3).start()

    wait_all(DQK)
    dqk_out[...] = recvs[DQK]
    wait_all(GG)
    gg_out[...] = recvs[GG]
    wait_all(GW)
    total = jnp.zeros((TOK, DV), F32)
    for b in range(SP):
        total = total + recvs[GW, pl.ds(b * TOK, TOK)].astype(F32)
    gw_out[...] = total
    for cc in range(4):
        to_core(far * 2 + 1 - core, cc, 3).wait_recv()
        at = pl.ds(pl.multiple_of(((z + 4 - cc) % 4) * BLK, BLK), BLK)
        gh_out[at] = (acc[pl.ds(cc * BLK, BLK)] + term(far, cc)).astype(BF16)

    def left_here(r, carry):
        for kind in range(8):
            sp_copy(kind, r, peer_of(r)).wait_send()
        return carry

    lax.fori_loop(1, SP, left_here, 0)

    def w_left(r, carry):
        w_copy(r).wait_send()
        return carry

    lax.fori_loop(1, TP, w_left, 0)
    for cc in range(4):
        for slot in range(3):
            to_chip(tp, cc, slot, right).wait_send()
        for slot in range(4):
            to_core(tp, cc, slot).wait_send()


def finish(dqk, gg, gh, gw, dq_out, dk_out, gf_out, gb_out, gh_out, gw_out):
    both = dqk[...]
    dq_out[...] = both[:, :DK].reshape(BATCH, TOK, DK)
    dk_out[...] = both[:, DK:].reshape(BATCH, TOK, DK)
    sums = gg[...].astype(F32)
    gf_out[...] = sums[:, :DK].reshape(BATCH, TOK, DK)
    gb_out[...] = sums[:, DK:].reshape(BATCH, TOK, DK)
    gh_out[...] = gh[...].reshape(BATCH, TOK, DV)
    gw_out[...] = gw[...]


def per_device(hidden, value_weight, queries, key_vectors, forward_decay, backward_decay, cotangent):
    in_hbm = pl.BlockSpec(memory_space=pltpu.HBM)
    vmem = pl.BlockSpec(memory_space=pltpu.VMEM)
    narrow = (BATCH, TOK, DK)
    wide = (ROWS, DV)
    sem = pltpu.SemaphoreType.DMA
    shape = jax.ShapeDtypeStruct
    rows_of = pl.pallas_call(
        kernel,
        out_shape=(shape(wide, BF16), shape(wide, BF16), shape(wide, BF16), shape((WIDTH // SP, DV), F32)),
        in_specs=[in_hbm] * 7,
        out_specs=(vmem,) * 4,
        scratch_shapes=[
            pltpu.VMEM((BATCH, TOK, WIDTH), BF16),
            pltpu.VMEM((WIDTH, DV), BF16),
            pltpu.VMEM(narrow, BF16),
            pltpu.VMEM(narrow, BF16),
            pltpu.VMEM(narrow, F32),
            pltpu.VMEM(narrow, F32),
            pltpu.VMEM((8, ROWS, DV), BF16),
            pltpu.VMEM((8, ROWS, DV), BF16),
            pltpu.VMEM(wide, BF16),
            pltpu.VMEM(wide, BF16),
            pltpu.VMEM(wide, F32),
            pltpu.VMEM(wide, F32),
            pltpu.VMEM((ROWS, BLK), BF16),
            pltpu.VMEM((2, NBLK * DV, DV), BF16),
            pltpu.VMEM((TP * ROWS, DV), BF16),
            pltpu.VMEM((TP * DV, DV), BF16),
            pltpu.VMEM(wide, F32),
            pltpu.VMEM((WIDTH, ROWS), BF16),
            sem((7,)),
            sem((8, SP)),
            sem((8, SP)),
            sem((8,)),
            sem((TP,)),
            sem((TP,)),
            sem((3, 4)),
            sem((3, 4)),
            sem((4, 4)),
            sem((4, 4)),
        ],
        compiler_params=pltpu.CompilerParams(
            collective_id=0, has_side_effects=True, vmem_limit_bytes=26 << 20
        ),
    )(
        *(
            pltpu.with_memory_space_constraint(operand, pltpu.HBM)
            for operand in (
                hidden,
                value_weight,
                queries.reshape(narrow),
                key_vectors.reshape(narrow),
                forward_decay.reshape(narrow),
                backward_decay.reshape(narrow),
                cotangent.reshape(wide),
            )
        )
    )
    outs = pl.pallas_call(
        finish,
        out_shape=(
            shape(narrow, BF16),
            shape(narrow, BF16),
            shape(narrow, F32),
            shape(narrow, F32),
            shape((BATCH, TOK, DV), BF16),
            shape((WIDTH // SP, DV), F32),
        ),
        in_specs=[vmem] * 4,
        out_specs=(vmem,) * 6,
        compiler_params=pltpu.CompilerParams(vmem_limit_bytes=16 << 20),
    )(*rows_of)
    heads = (BATCH, 1, TOK, DK)
    return tuple(out.reshape(heads) for out in outs[:4]) + tuple(outs[4:])


def solution(mesh):
    spread = P(None, "tp", "sp", None)
    return jax.shard_map(
        per_device,
        mesh=mesh,
        in_specs=(
            P(None, "sp", None),
            P(None, "tp"),
            spread,
            spread,
            spread,
            spread,
            P(None, "sp", "tp"),
        ),
        out_specs=(spread, spread, spread, spread, P(None, "sp", "tp"), P("sp", "tp")),
        check_vma=False,
    )
```

```python
import functools

import jax
import jax.numpy as jnp
from jax import lax
from jax.experimental import pallas as pl
from jax.experimental.pallas import tpu as pltpu
from jax.sharding import PartitionSpec as P

MESH = pl.DeviceIdType.MESH
F32, BF16 = jnp.float32, jnp.bfloat16
SP, TP = 16, 8
BATCH, TOK, DK, DV, WIDTH = 16, 64, 64, 128, 1024
ROWS = BATCH * TOK
BLK = 256
NBLK = ROWS // BLK
STEP = 2.0**-16
QK, DEC, DO, VV, DVT, DQK, GG, GW = range(8)


def iota(shape, axis):
    return lax.broadcasted_iota(jnp.int32, shape, axis)


def dot(a, b):
    return lax.dot_general(a, b, (((1,), (0,)), ((), ())), preferred_element_type=F32)


def dot_nt(a, b):
    return lax.dot_general(a, b, (((1,), (1,)), ((), ())), preferred_element_type=F32)


def dot_tn(a, b):
    return lax.dot_general(a, b, (((0,), (0,)), ((), ())), preferred_element_type=F32)


def hi_lo(x):
    hi = x.astype(BF16)
    lo = (x - hi.astype(F32)).astype(BF16)
    return jnp.concatenate([hi, lo], axis=1)


def tri(group):
    r, c = iota((BLK, BLK), 0), iota((BLK, BLK), 1)
    keep = r >= c
    if group < BLK:
        keep = keep & (r // group == c // group)
    return jnp.where(keep, 1.0, 0.0).astype(BF16)


def tile(ref, index):
    return ref.at[pl.ds(pl.multiple_of(index * TOK, TOK), TOK)]


def kernel(
    hidden,
    weight,
    q_hbm,
    k_hbm,
    df_hbm,
    db_hbm,
    cot,
    dq_out,
    dk_out,
    gf_out,
    gb_out,
    gh_out,
    gw_out,
    hid,
    w,
    q_in,
    k_in,
    df_in,
    db_in,
    sends,
    recvs,
    qhat,
    khat,
    grow,
    gterm,
    scores,
    parts,
    dall,
    wx,
    acc,
    hid_t,
    in_sem,
    ss,
    rs,
    loc_sem,
    wss,
    wrs,
    xss,
    xrs,
    pss,
    prs,
):
    me = lax.axis_index("sp")
    tp = lax.axis_index("tp")
    y, z = me % 4, me // 4
    core, xc = tp % 2, tp // 2
    barrier = pltpu.get_barrier_semaphore()

    def greet_sp(r, carry):
        pl.semaphore_signal(
            barrier, inc=1, device_id={"sp": (me + r) % SP}, device_id_type=MESH
        )
        return carry

    def greet_tp(r, carry):
        pl.semaphore_signal(
            barrier, inc=1, device_id={"tp": (tp + r) % TP}, device_id_type=MESH
        )
        return carry

    lax.fori_loop(1, SP, greet_sp, 0)
    lax.fori_loop(1, TP, greet_tp, 0)

    loads = [
        pltpu.make_async_copy(df_hbm, df_in, in_sem.at[2]),
        pltpu.make_async_copy(db_hbm, db_in, in_sem.at[3]),
        pltpu.make_async_copy(q_hbm, q_in, in_sem.at[0]),
        pltpu.make_async_copy(k_hbm, k_in, in_sem.at[1]),
        pltpu.make_async_copy(cot, sends.at[DO], in_sem.at[4]),
        pltpu.make_async_copy(weight, w, in_sem.at[5]),
        pltpu.make_async_copy(hidden, hid, in_sem.at[6]),
    ]
    for load in loads:
        load.start()

    def peer_of(r):
        m = (r * 7) % SP
        return ((z + m // 4) % 4) * 4 + (y + m % 4) % 4

    def landing(kind, frm):
        if kind == DVT:
            return dall.at[pl.ds(pl.multiple_of(tp * ROWS + frm * TOK, TOK), TOK)]
        return tile(recvs.at[kind], frm)

    def sp_copy(kind, r, to):
        return pltpu.make_async_remote_copy(
            src_ref=tile(sends.at[kind], to),
            dst_ref=landing(kind, me),
            send_sem=ss.at[kind, r],
            recv_sem=rs.at[kind, me],
            device_id={"sp": to},
            device_id_type=MESH,
        )

    def sp_wait(kind, r, frm):
        pltpu.make_async_remote_copy(
            src_ref=landing(kind, frm),
            dst_ref=landing(kind, frm),
            send_sem=ss.at[kind, r],
            recv_sem=rs.at[kind, frm],
            device_id={"sp": frm},
            device_id_type=MESH,
        ).wait_recv()

    def own_copy(kind):
        return pltpu.make_async_copy(
            tile(sends.at[kind], me), landing(kind, me), loc_sem.at[kind]
        )

    def send_all(kind):
        def body(r, carry):
            sp_copy(kind, r, peer_of(r)).start()
            return carry

        lax.fori_loop(1, SP, body, 0)
        own_copy(kind).start()

    def wait_all(kind):
        def body(r, carry):
            sp_wait(kind, r, peer_of(r))
            return carry

        lax.fori_loop(1, SP, body, 0)
        own_copy(kind).wait()

    def send_block(kind, jj, blk):
        for i in range(4):
            if jj == 0 and i == 0:
                own_copy(kind).start()
            else:
                sp_copy(kind, jj * 4 + i, blk * 4 + (y + i) % 4).start()

    def wait_plane(kind, jj, plane):
        for i in range(4):
            if jj == 0 and i == 0:
                own_copy(kind).wait()
            else:
                sp_wait(kind, jj * 4 + i, plane * 4 + (y + i) % 4)

    loads[0].wait()
    loads[1].wait()
    low = tri(TOK)
    for b in range(NBLK):
        span = pl.ds(b * 4, 4)
        both = jnp.concatenate(
            [df_in[span].reshape(BLK, DK), db_in[span].reshape(BLK, DK)], axis=1
        )
        run = dot(low, hi_lo(both))
        steps = jnp.round((run[:, :DV] + run[:, DV:]) * (1.0 / STEP))
        before = jnp.where(iota((BLK, DV), 0) % TOK == 0, 0.0, pltpu.roll(steps, 1, 0))
        sends[DEC, pl.ds(b * BLK, BLK)] = ((steps - before) * STEP).astype(BF16)
    loads[2].wait()
    loads[3].wait()
    sends[QK] = jnp.concatenate(
        [q_in[...].reshape(ROWS, DK), k_in[...].reshape(ROWS, DK)], axis=1
    )
    loads[4].wait()
    loads[5].wait()
    pl.semaphore_wait(barrier, SP + TP - 2)
    send_all(DEC)
    send_all(QK)
    send_all(DO)

    def w_copy(r):
        to = (tp + r) % TP
        return pltpu.make_async_remote_copy(
            src_ref=w.at[pl.ds(pl.multiple_of(to * DV, DV), DV)],
            dst_ref=wx.at[pl.ds(pl.multiple_of(tp * DV, DV), DV)],
            send_sem=wss.at[r],
            recv_sem=wrs.at[r],
            device_id={"tp": to},
            device_id_type=MESH,
        )

    def w_send(r, carry):
        w_copy(r).start()
        return carry

    lax.fori_loop(1, TP, w_send, 0)
    own_w = pltpu.make_async_copy(
        w.at[pl.ds(pl.multiple_of(tp * DV, DV), DV)],
        wx.at[pl.ds(pl.multiple_of(tp * DV, DV), DV)],
        wrs.at[0],
    )
    own_w.start()

    loads[6].wait()
    for b in range(NBLK):
        rows = hid[pl.ds(b * 4, 4)].reshape(BLK, WIDTH)
        sends[VV, pl.ds(b * BLK, BLK)] = dot(rows, w[...]).astype(BF16)
    send_all(VV)

    def turn(t, carry):
        at = pl.ds(pl.multiple_of(t * 128, 128), 128)
        hid_t[:, at] = hid[pl.ds(t * 2, 2)].reshape(128, WIDTH).T
        return carry

    lax.fori_loop(0, ROWS // 128, turn, 0)

    wait_all(DEC)
    lane_f = iota((BLK, DV), 1) < DK
    full = tri(BLK)
    base = jnp.zeros((1, DV), F32)
    cums = []
    for b in range(NBLK):
        d = recvs[DEC, pl.ds(b * BLK, BLK)]
        inside = dot(full, d) + base
        base = inside[BLK - 1 :, :]
        cums.append(jnp.where(lane_f, inside, d.astype(F32) - inside))
    wait_all(QK)
    r_, c_ = iota((BLK, BLK), 0), iota((BLK, BLK), 1)
    zero16 = jnp.zeros((), BF16)
    for b in range(NBLK):
        at = pl.ds(b * BLK, BLK)
        growth = jnp.exp(cums[b])
        shrink = jnp.exp(-cums[b])
        qk = recvs[QK, at].astype(F32)
        kq = pltpu.roll(qk, DK, 1)
        qh = (jnp.where(lane_f, qk, kq) * growth).astype(BF16)
        kh = (jnp.where(lane_f, kq, qk) * shrink).astype(BF16)
        qhat[at] = qh
        khat[at] = kh
        grow[at] = growth
        fwd = dot_nt(jnp.where(lane_f, kh, zero16), qh)
        bwd = dot_nt(jnp.where(lane_f, zero16, kh), qh)
        both = jnp.where(r_ <= c_, fwd, 0.0) + jnp.where(r_ >= c_, bwd, 0.0)
        scores[at] = both.astype(BF16)
    row_f = iota((DV, DV), 0) < DK

    def others(pieces):
        zero = jnp.zeros((DV, DV), F32)
        after, before = [zero] * NBLK, [zero] * NBLK
        for b in range(NBLK - 2, -1, -1):
            after[b] = after[b + 1] + pieces[b + 1]
        for b in range(1, NBLK):
            before[b] = before[b - 1] + pieces[b - 1]
        return after, before

    wait_all(DO)
    pieces = [
        dot_tn(qhat[pl.ds(b * BLK, BLK)], recvs[DO, pl.ds(b * BLK, BLK)]) for b in range(NBLK)
    ]
    after, before = others(pieces)
    for b in range(NBLK):
        parts[0, pl.ds(b * DV, DV)] = jnp.where(row_f, after[b], before[b]).astype(BF16)
    for jj in range(NBLK):
        blk = (z + jj) % NBLK
        at = pl.ds(pl.multiple_of(blk * BLK, BLK), BLK)
        pat = pl.ds(pl.multiple_of(blk * DV, DV), DV)
        dv = dot(khat[at], parts[0, pat]) + dot(scores[at], recvs[DO, at])
        sends[DVT, at] = dv.astype(BF16)
        send_block(DVT, jj, blk)

    right, left, far = (xc + 1) % 4, (xc + 3) % 4, (xc + 2) % 4

    def piece(head, cc):
        row = head * ROWS + ((z + 4 - cc) % 4) * BLK
        return dall.at[pl.ds(pl.multiple_of(row, BLK), BLK)]

    def hop(head, cc, sems_s, sems_r, slot, to):
        return pltpu.make_async_remote_copy(
            src_ref=piece(head, cc),
            dst_ref=piece(head, cc),
            send_sem=sems_s.at[slot, cc],
            recv_sem=sems_r.at[slot, cc],
            device_id={"tp": to},
            device_id_type=MESH,
        )

    def to_chip(head, cc, slot, chip):
        return hop(head, cc, xss, xrs, slot, chip * 2 + core)

    def to_core(head, cc, slot):
        return hop(head, cc, pss, prs, slot, xc * 2 + 1 - core)

    def first_hops(cc):
        wait_plane(DVT, cc, (z + 4 - cc) % 4)
        to_chip(tp, cc, 0, right).start()
        to_chip(tp, cc, 1, left).start()
        to_core(tp, cc, 0).start()

    wait_all(VV)
    pieces = [
        dot_tn(khat[pl.ds(b * BLK, BLK)], recvs[VV, pl.ds(b * BLK, BLK)]) for b in range(NBLK)
    ]
    after, before = others(pieces)
    for b in range(NBLK):
        parts[1, pl.ds(b * DV, DV)] = jnp.where(row_f, before[b], after[b]).astype(BF16)
    for jj in range(NBLK):
        blk = (z + jj) % NBLK
        at = pl.ds(pl.multiple_of(blk * BLK, BLK), BLK)
        pat = pl.ds(pl.multiple_of(blk * DV, DV), DV)
        qh, kh, do, v = qhat[at], khat[at], recvs[DO, at], recvs[VV, at]
        growth = grow[at]
        s = dot_nt(do, v).astype(BF16)
        st = dot_nt(v, do).astype(BF16)
        x = dot_nt(do, parts[1, pat])
        x = x + dot(jnp.where(r_ >= c_, s, zero16), jnp.where(lane_f, kh, zero16))
        x = x + dot(jnp.where(r_ <= c_, s, zero16), jnp.where(lane_f, zero16, kh))
        yk = dot_nt(v, parts[0, pat])
        yk = yk + dot(jnp.where(r_ <= c_, st, zero16), jnp.where(lane_f, qh, zero16))
        yk = yk + dot(jnp.where(r_ >= c_, st, zero16), jnp.where(lane_f, zero16, qh))
        gterm[at] = qh.astype(F32) * x - kh.astype(F32) * yk
        dq2 = x * growth
        dk2 = yk / growth
        dq2 = dq2 + pltpu.roll(dq2, DK, 1)
        dk2 = dk2 + pltpu.roll(dk2, DK, 1)
        sends[DQK, at] = jnp.where(lane_f, dq2, dk2).astype(BF16)
        send_block(DQK, jj, blk)
        first_hops(jj)
    base = jnp.zeros((1, DV), F32)
    for b in range(NBLK):
        at = pl.ds(b * BLK, BLK)
        g = gterm[at]
        run = dot(full, hi_lo(g))
        run = run[:, :DV] + run[:, DV:] + base
        base = run[BLK - 1 :, :]
        sends[GG, at] = jnp.where(lane_f, g - run, run).astype(BF16)

    drows = dall[pl.ds(pl.multiple_of(tp * ROWS, ROWS), ROWS)]
    for b in range(NBLK):
        at = pl.ds(b * BLK, BLK)
        sends[GW, at] = dot(hid_t[at], drows).astype(BF16)
    send_all(GW)
    send_all(GG)

    def w_arrived(r, carry):
        frm = (tp + TP - r) % TP
        spot = wx.at[pl.ds(pl.multiple_of(frm * DV, DV), DV)]
        pltpu.make_async_remote_copy(
            src_ref=spot,
            dst_ref=spot,
            send_sem=wss.at[r],
            recv_sem=wrs.at[r],
            device_id={"tp": frm},
            device_id_type=MESH,
        ).wait_recv()
        return carry

    lax.fori_loop(1, TP, w_arrived, 0)
    own_w.wait()

    def term(chip, cc):
        total = None
        for c in range(2):
            head = chip * 2 + c
            row = head * ROWS + ((z + 4 - cc) % 4) * BLK
            rows = dall[pl.ds(pl.multiple_of(row, BLK), BLK)]
            part = dot_nt(rows, wx[pl.ds(pl.multiple_of(head * DV, DV), DV)])
            total = part if total is None else total + part
        return total

    for cc in range(4):
        head_l, head_r = left * 2 + core, right * 2 + core
        to_chip(head_l, cc, 0, left).wait_recv()
        if cc % 2 == 0:
            to_chip(head_l, cc, 2, right).start()
        to_core(head_l, cc, 1).start()
        to_chip(head_r, cc, 1, right).wait_recv()
        if cc % 2 == 1:
            to_chip(head_r, cc, 2, left).start()
        to_core(head_r, cc, 2).start()
    for cc in range(4):
        for slot, chip in ((0, xc), (1, left), (2, right)):
            to_core(chip * 2 + 1 - core, cc, slot).wait_recv()
        acc[pl.ds(cc * BLK, BLK)] = term(xc, cc) + term(left, cc) + term(right, cc)
    for cc in range(4):
        to_chip(far * 2 + core, cc, 2, far).wait_recv()
        to_core(far * 2 + core, cc, 3).start()

    wait_all(DQK)
    for b in range(NBLK):
        both, span = recvs[DQK, pl.ds(b * BLK, BLK)], pl.ds(b * 4, 4)
        dq_out[span] = both[:, :DK].reshape(4, TOK, DK)
        dk_out[span] = both[:, DK:].reshape(4, TOK, DK)
    wait_all(GG)
    for b in range(NBLK):
        both, span = recvs[GG, pl.ds(b * BLK, BLK)].astype(F32), pl.ds(b * 4, 4)
        gf_out[span] = both[:, :DK].reshape(4, TOK, DK)
        gb_out[span] = both[:, DK:].reshape(4, TOK, DK)
    wait_all(GW)
    total = jnp.zeros((TOK, DV), F32)
    for b in range(SP):
        total = total + recvs[GW, pl.ds(b * TOK, TOK)].astype(F32)
    gw_out[...] = total
    for cc in range(4):
        to_core(far * 2 + 1 - core, cc, 3).wait_recv()
        at = pl.ds(pl.multiple_of(((z + 4 - cc) % 4) * BLK, BLK), BLK)
        gh_out[at] = (acc[pl.ds(cc * BLK, BLK)] + term(far, cc)).astype(BF16)

    def left_here(r, carry):
        for kind in range(8):
            sp_copy(kind, r, peer_of(r)).wait_send()
        return carry

    lax.fori_loop(1, SP, left_here, 0)

    def w_left(r, carry):
        w_copy(r).wait_send()
        return carry

    lax.fori_loop(1, TP, w_left, 0)
    for cc in range(4):
        for slot in range(3):
            to_chip(tp, cc, slot, right).wait_send()
        for slot in range(4):
            to_core(tp, cc, slot).wait_send()


def finish(*refs):
    out_sem = refs[-1]
    copies = [pltpu.make_async_copy(refs[i], refs[i + 6], out_sem.at[i]) for i in (2, 3, 0, 1, 4, 5)]
    for copy in copies:
        copy.start()
    for copy in copies:
        copy.wait()


def per_device(hidden, value_weight, queries, key_vectors, forward_decay, backward_decay, cotangent):
    in_hbm = pl.BlockSpec(memory_space=pltpu.HBM)
    vmem = pl.BlockSpec(memory_space=pltpu.VMEM)
    narrow = (BATCH, TOK, DK)
    wide = (ROWS, DV)
    sem = pltpu.SemaphoreType.DMA
    shape = jax.ShapeDtypeStruct
    rows_of = pl.pallas_call(
        kernel,
        out_shape=(
            shape(narrow, BF16),
            shape(narrow, BF16),
            shape(narrow, F32),
            shape(narrow, F32),
            shape(wide, BF16),
            shape((WIDTH // SP, DV), F32),
        ),
        in_specs=[in_hbm] * 7,
        out_specs=(vmem,) * 6,
        scratch_shapes=[
            pltpu.VMEM((BATCH, TOK, WIDTH), BF16),
            pltpu.VMEM((WIDTH, DV), BF16),
            pltpu.VMEM(narrow, BF16),
            pltpu.VMEM(narrow, BF16),
            pltpu.VMEM(narrow, F32),
            pltpu.VMEM(narrow, F32),
            pltpu.VMEM((8, ROWS, DV), BF16),
            pltpu.VMEM((8, ROWS, DV), BF16),
            pltpu.VMEM(wide, BF16),
            pltpu.VMEM(wide, BF16),
            pltpu.VMEM(wide, F32),
            pltpu.VMEM(wide, F32),
            pltpu.VMEM((ROWS, BLK), BF16),
            pltpu.VMEM((2, NBLK * DV, DV), BF16),
            pltpu.VMEM((TP * ROWS, DV), BF16),
            pltpu.VMEM((TP * DV, DV), BF16),
            pltpu.VMEM(wide, F32),
            pltpu.VMEM((WIDTH, ROWS), BF16),
            sem((7,)),
            sem((8, SP)),
            sem((8, SP)),
            sem((8,)),
            sem((TP,)),
            sem((TP,)),
            sem((3, 4)),
            sem((3, 4)),
            sem((4, 4)),
            sem((4, 4)),
        ],
        compiler_params=pltpu.CompilerParams(
            collective_id=0, has_side_effects=True, vmem_limit_bytes=26 << 20
        ),
    )(
        *(
            pltpu.with_memory_space_constraint(operand, pltpu.HBM)
            for operand in (
                hidden,
                value_weight,
                queries.reshape(narrow),
                key_vectors.reshape(narrow),
                forward_decay.reshape(narrow),
                backward_decay.reshape(narrow),
                cotangent.reshape(wide),
            )
        )
    )
    outs = pl.pallas_call(
        finish,
        out_shape=(
            shape(narrow, BF16),
            shape(narrow, BF16),
            shape(narrow, F32),
            shape(narrow, F32),
            shape(wide, BF16),
            shape((WIDTH // SP, DV), F32),
        ),
        in_specs=[vmem] * 6,
        out_specs=(in_hbm,) * 6,
        scratch_shapes=[sem((6,))],
        compiler_params=pltpu.CompilerParams(vmem_limit_bytes=16 << 20),
    )(*rows_of)
    heads = (BATCH, 1, TOK, DK)
    return tuple(out.reshape(heads) for out in outs[:4]) + (outs[4].reshape(BATCH, TOK, DV), outs[5])


def solution(mesh):
    spread = P(None, "tp", "sp", None)
    return jax.shard_map(
        per_device,
        mesh=mesh,
        in_specs=(
            P(None, "sp", None),
            P(None, "tp"),
            spread,
            spread,
            spread,
            spread,
            P(None, "sp", "tp"),
        ),
        out_specs=(spread, spread, spread, spread, P(None, "sp", "tp"), P("sp", "tp")),
        check_vma=False,
    )
```

```python
import functools

import jax
import jax.numpy as jnp
from jax import lax
from jax.experimental import pallas as pl
from jax.experimental.pallas import tpu as pltpu
from jax.sharding import PartitionSpec as P

MESH = pl.DeviceIdType.MESH
F32, BF16 = jnp.float32, jnp.bfloat16
SP, TP = 16, 8
BATCH, TOK, DK, DV, WIDTH = 16, 64, 64, 128, 1024
ROWS = BATCH * TOK
BLK = 256
NBLK = ROWS // BLK
STEP = 2.0**-16
QK, DEC, DO, VV, DVT, DQK, GG, GW = range(8)


def iota(shape, axis):
    return lax.broadcasted_iota(jnp.int32, shape, axis)


def dot(a, b):
    return lax.dot_general(a, b, (((1,), (0,)), ((), ())), preferred_element_type=F32)


def dot_nt(a, b):
    return lax.dot_general(a, b, (((1,), (1,)), ((), ())), preferred_element_type=F32)


def dot_tn(a, b):
    return lax.dot_general(a, b, (((0,), (0,)), ((), ())), preferred_element_type=F32)


def hi_lo(x):
    hi = x.astype(BF16)
    lo = (x - hi.astype(F32)).astype(BF16)
    return jnp.concatenate([hi, lo], axis=1)


def tri(group):
    r, c = iota((BLK, BLK), 0), iota((BLK, BLK), 1)
    keep = r >= c
    if group < BLK:
        keep = keep & (r // group == c // group)
    return jnp.where(keep, 1.0, 0.0).astype(BF16)


def tile(ref, index):
    return ref.at[pl.ds(pl.multiple_of(index * TOK, TOK), TOK)]


def kernel(
    hidden,
    weight,
    q_hbm,
    k_hbm,
    df_hbm,
    db_hbm,
    cot,
    dq_out,
    dk_out,
    gf_out,
    gb_out,
    gh_out,
    gw_out,
    hid,
    w,
    q_in,
    k_in,
    df_in,
    db_in,
    sends,
    recvs,
    qhat,
    khat,
    grow,
    gterm,
    scores,
    parts,
    dall,
    wx,
    acc,
    hid_t,
    in_sem,
    ss,
    rs,
    loc_sem,
    wss,
    wrs,
    xss,
    xrs,
    pss,
    prs,
):
    me = lax.axis_index("sp")
    tp = lax.axis_index("tp")
    y, z = me % 4, me // 4
    core, xc = tp % 2, tp // 2
    barrier = pltpu.get_barrier_semaphore()

    def greet_sp(r, carry):
        pl.semaphore_signal(
            barrier, inc=1, device_id={"sp": (me + r) % SP}, device_id_type=MESH
        )
        return carry

    def greet_tp(r, carry):
        pl.semaphore_signal(
            barrier, inc=1, device_id={"tp": (tp + r) % TP}, device_id_type=MESH
        )
        return carry

    lax.fori_loop(1, SP, greet_sp, 0)
    lax.fori_loop(1, TP, greet_tp, 0)

    loads = [
        pltpu.make_async_copy(df_hbm, df_in, in_sem.at[2]),
        pltpu.make_async_copy(db_hbm, db_in, in_sem.at[3]),
        pltpu.make_async_copy(q_hbm, q_in, in_sem.at[0]),
        pltpu.make_async_copy(k_hbm, k_in, in_sem.at[1]),
        pltpu.make_async_copy(cot, sends.at[DO], in_sem.at[4]),
        pltpu.make_async_copy(weight, w, in_sem.at[5]),
        pltpu.make_async_copy(hidden, hid, in_sem.at[6]),
    ]
    for load in loads:
        load.start()

    def peer_of(r):
        m = (r * 7) % SP
        return ((z + m // 4) % 4) * 4 + (y + m % 4) % 4

    def landing(kind, frm):
        if kind == DVT:
            return dall.at[pl.ds(pl.multiple_of(tp * ROWS + frm * TOK, TOK), TOK)]
        return tile(recvs.at[kind], frm)

    def sp_copy(kind, r, to):
        return pltpu.make_async_remote_copy(
            src_ref=tile(sends.at[kind], to),
            dst_ref=landing(kind, me),
            send_sem=ss.at[kind, r],
            recv_sem=rs.at[kind, me],
            device_id={"sp": to},
            device_id_type=MESH,
        )

    def sp_wait(kind, r, frm):
        pltpu.make_async_remote_copy(
            src_ref=landing(kind, frm),
            dst_ref=landing(kind, frm),
            send_sem=ss.at[kind, r],
            recv_sem=rs.at[kind, frm],
            device_id={"sp": frm},
            device_id_type=MESH,
        ).wait_recv()

    def own_copy(kind):
        return pltpu.make_async_copy(
            tile(sends.at[kind], me), landing(kind, me), loc_sem.at[kind]
        )

    def send_all(kind):
        def body(r, carry):
            sp_copy(kind, r, peer_of(r)).start()
            return carry

        lax.fori_loop(1, SP, body, 0)
        own_copy(kind).start()

    def wait_all(kind):
        def body(r, carry):
            sp_wait(kind, r, peer_of(r))
            return carry

        lax.fori_loop(1, SP, body, 0)
        own_copy(kind).wait()

    def send_block(kind, jj, blk):
        for i in range(4):
            if jj == 0 and i == 0:
                own_copy(kind).start()
            else:
                sp_copy(kind, jj * 4 + i, blk * 4 + (y + i) % 4).start()

    def wait_plane(kind, jj, plane):
        for i in range(4):
            if jj == 0 and i == 0:
                own_copy(kind).wait()
            else:
                sp_wait(kind, jj * 4 + i, plane * 4 + (y + i) % 4)

    loads[0].wait()
    loads[1].wait()
    low = tri(TOK)
    for b in range(NBLK):
        span = pl.ds(b * 4, 4)
        both = jnp.concatenate(
            [df_in[span].reshape(BLK, DK), db_in[span].reshape(BLK, DK)], axis=1
        )
        run = dot(low, hi_lo(both))
        steps = jnp.round((run[:, :DV] + run[:, DV:]) * (1.0 / STEP))
        before = jnp.where(iota((BLK, DV), 0) % TOK == 0, 0.0, pltpu.roll(steps, 1, 0))
        sends[DEC, pl.ds(b * BLK, BLK)] = ((steps - before) * STEP).astype(BF16)
    loads[2].wait()
    loads[3].wait()
    sends[QK] = jnp.concatenate(
        [q_in[...].reshape(ROWS, DK), k_in[...].reshape(ROWS, DK)], axis=1
    )
    loads[4].wait()
    loads[5].wait()
    pl.semaphore_wait(barrier, SP + TP - 2)
    send_all(DEC)
    send_all(QK)
    send_all(DO)

    def w_copy(r):
        to = (tp + r) % TP
        return pltpu.make_async_remote_copy(
            src_ref=w.at[pl.ds(pl.multiple_of(to * DV, DV), DV)],
            dst_ref=wx.at[pl.ds(pl.multiple_of(tp * DV, DV), DV)],
            send_sem=wss.at[r],
            recv_sem=wrs.at[r],
            device_id={"tp": to},
            device_id_type=MESH,
        )

    def w_send(r, carry):
        w_copy(r).start()
        return carry

    own_w = pltpu.make_async_copy(
        w.at[pl.ds(pl.multiple_of(tp * DV, DV), DV)],
        wx.at[pl.ds(pl.multiple_of(tp * DV, DV), DV)],
        wrs.at[0],
    )
    own_w.start()

    loads[6].wait()
    for b in range(NBLK):
        rows = hid[pl.ds(b * 4, 4)].reshape(BLK, WIDTH)
        sends[VV, pl.ds(b * BLK, BLK)] = dot(rows, w[...]).astype(BF16)
    send_all(VV)
    lax.fori_loop(1, TP, w_send, 0)

    def turn(t, carry):
        at = pl.ds(pl.multiple_of(t * 128, 128), 128)
        hid_t[:, at] = hid[pl.ds(t * 2, 2)].reshape(128, WIDTH).T
        return carry

    lax.fori_loop(0, ROWS // 128, turn, 0)

    wait_all(DEC)
    lane_f = iota((BLK, DV), 1) < DK
    full = tri(BLK)
    base = jnp.zeros((1, DV), F32)
    cums = []
    for b in range(NBLK):
        d = recvs[DEC, pl.ds(b * BLK, BLK)]
        inside = dot(full, d) + base
        base = inside[BLK - 1 :, :]
        cums.append(jnp.where(lane_f, inside, d.astype(F32) - inside))
    wait_all(QK)
    r_, c_ = iota((BLK, BLK), 0), iota((BLK, BLK), 1)
    zero16 = jnp.zeros((), BF16)
    for b in range(NBLK):
        at = pl.ds(b * BLK, BLK)
        growth = jnp.exp(cums[b])
        shrink = jnp.exp(-cums[b])
        qk = recvs[QK, at].astype(F32)
        kq = pltpu.roll(qk, DK, 1)
        qh = (jnp.where(lane_f, qk, kq) * growth).astype(BF16)
        kh = (jnp.where(lane_f, kq, qk) * shrink).astype(BF16)
        qhat[at] = qh
        khat[at] = kh
        grow[at] = growth
        fwd = dot_nt(jnp.where(lane_f, kh, zero16), qh)
        bwd = dot_nt(jnp.where(lane_f, zero16, kh), qh)
        both = jnp.where(r_ <= c_, fwd, 0.0) + jnp.where(r_ >= c_, bwd, 0.0)
        scores[at] = both.astype(BF16)
    row_f = iota((DV, DV), 0) < DK

    def others(pieces):
        zero = jnp.zeros((DV, DV), F32)
        after, before = [zero] * NBLK, [zero] * NBLK
        for b in range(NBLK - 2, -1, -1):
            after[b] = after[b + 1] + pieces[b + 1]
        for b in range(1, NBLK):
            before[b] = before[b - 1] + pieces[b - 1]
        return after, before

    wait_all(DO)
    pieces = [
        dot_tn(qhat[pl.ds(b * BLK, BLK)], recvs[DO, pl.ds(b * BLK, BLK)]) for b in range(NBLK)
    ]
    after, before = others(pieces)
    for b in range(NBLK):
        parts[0, pl.ds(b * DV, DV)] = jnp.where(row_f, after[b], before[b]).astype(BF16)
    for jj in range(NBLK):
        blk = (z + jj) % NBLK
        at = pl.ds(pl.multiple_of(blk * BLK, BLK), BLK)
        pat = pl.ds(pl.multiple_of(blk * DV, DV), DV)
        dv = dot(khat[at], parts[0, pat]) + dot(scores[at], recvs[DO, at])
        sends[DVT, at] = dv.astype(BF16)
        send_block(DVT, jj, blk)

    right, left, far = (xc + 1) % 4, (xc + 3) % 4, (xc + 2) % 4

    def piece(head, cc):
        row = head * ROWS + ((z + 4 - cc) % 4) * BLK
        return dall.at[pl.ds(pl.multiple_of(row, BLK), BLK)]

    def hop(head, cc, sems_s, sems_r, slot, to):
        return pltpu.make_async_remote_copy(
            src_ref=piece(head, cc),
            dst_ref=piece(head, cc),
            send_sem=sems_s.at[slot, cc],
            recv_sem=sems_r.at[slot, cc],
            device_id={"tp": to},
            device_id_type=MESH,
        )

    def to_chip(head, cc, slot, chip):
        return hop(head, cc, xss, xrs, slot, chip * 2 + core)

    def to_core(head, cc, slot):
        return hop(head, cc, pss, prs, slot, xc * 2 + 1 - core)

    def first_hops(cc):
        wait_plane(DVT, cc, (z + 4 - cc) % 4)
        to_chip(tp, cc, 0, right).start()
        to_chip(tp, cc, 1, left).start()
        to_core(tp, cc, 0).start()

    wait_all(VV)
    pieces = [
        dot_tn(khat[pl.ds(b * BLK, BLK)], recvs[VV, pl.ds(b * BLK, BLK)]) for b in range(NBLK)
    ]
    after, before = others(pieces)
    for b in range(NBLK):
        parts[1, pl.ds(b * DV, DV)] = jnp.where(row_f, before[b], after[b]).astype(BF16)
    for jj in range(NBLK):
        blk = (z + jj) % NBLK
        at = pl.ds(pl.multiple_of(blk * BLK, BLK), BLK)
        pat = pl.ds(pl.multiple_of(blk * DV, DV), DV)
        qh, kh, do, v = qhat[at], khat[at], recvs[DO, at], recvs[VV, at]
        growth = grow[at]
        s = dot_nt(do, v).astype(BF16)
        st = dot_nt(v, do).astype(BF16)
        x = dot_nt(do, parts[1, pat])
        x = x + dot(jnp.where(r_ >= c_, s, zero16), jnp.where(lane_f, kh, zero16))
        x = x + dot(jnp.where(r_ <= c_, s, zero16), jnp.where(lane_f, zero16, kh))
        yk = dot_nt(v, parts[0, pat])
        yk = yk + dot(jnp.where(r_ <= c_, st, zero16), jnp.where(lane_f, qh, zero16))
        yk = yk + dot(jnp.where(r_ >= c_, st, zero16), jnp.where(lane_f, zero16, qh))
        gterm[at] = qh.astype(F32) * x - kh.astype(F32) * yk
        dq2 = x * growth
        dk2 = yk / growth
        dq2 = dq2 + pltpu.roll(dq2, DK, 1)
        dk2 = dk2 + pltpu.roll(dk2, DK, 1)
        sends[DQK, at] = jnp.where(lane_f, dq2, dk2).astype(BF16)
        send_block(DQK, jj, blk)
        first_hops(jj)
    base = jnp.zeros((1, DV), F32)
    for b in range(NBLK):
        at = pl.ds(b * BLK, BLK)
        g = gterm[at]
        run = dot(full, hi_lo(g))
        run = run[:, :DV] + run[:, DV:] + base
        base = run[BLK - 1 :, :]
        sends[GG, at] = jnp.where(lane_f, g - run, run).astype(BF16)

    drows = dall[pl.ds(pl.multiple_of(tp * ROWS, ROWS), ROWS)]
    for b in range(NBLK):
        at = pl.ds(b * BLK, BLK)
        sends[GW, at] = dot(hid_t[at], drows).astype(BF16)
    send_all(GW)
    send_all(GG)

    def w_arrived(r, carry):
        frm = (tp + TP - r) % TP
        spot = wx.at[pl.ds(pl.multiple_of(frm * DV, DV), DV)]
        pltpu.make_async_remote_copy(
            src_ref=spot,
            dst_ref=spot,
            send_sem=wss.at[r],
            recv_sem=wrs.at[r],
            device_id={"tp": frm},
            device_id_type=MESH,
        ).wait_recv()
        return carry

    lax.fori_loop(1, TP, w_arrived, 0)
    own_w.wait()

    def term(chip, cc):
        rows, cols = [], []
        for head in (chip * 2, chip * 2 + 1):
            row = head * ROWS + ((z + 4 - cc) % 4) * BLK
            rows.append(dall[pl.ds(pl.multiple_of(row, BLK), BLK)])
            cols.append(wx[pl.ds(pl.multiple_of(head * DV, DV), DV)])
        return dot_nt(jnp.concatenate(rows, axis=1), jnp.concatenate(cols, axis=1))

    for cc in range(4):
        head_l, head_r = left * 2 + core, right * 2 + core
        to_chip(head_l, cc, 0, left).wait_recv()
        if cc % 2 == 0:
            to_chip(head_l, cc, 2, right).start()
        to_core(head_l, cc, 1).start()
        to_chip(head_r, cc, 1, right).wait_recv()
        if cc % 2 == 1:
            to_chip(head_r, cc, 2, left).start()
        to_core(head_r, cc, 2).start()
    for cc in range(4):
        for slot, chip in ((0, xc), (1, left), (2, right)):
            to_core(chip * 2 + 1 - core, cc, slot).wait_recv()
        acc[pl.ds(cc * BLK, BLK)] = term(xc, cc) + term(left, cc) + term(right, cc)
    for cc in range(4):
        to_chip(far * 2 + core, cc, 2, far).wait_recv()
        to_core(far * 2 + core, cc, 3).start()

    wait_all(DQK)
    for b in range(NBLK):
        both, span = recvs[DQK, pl.ds(b * BLK, BLK)], pl.ds(b * 4, 4)
        dq_out[span] = both[:, :DK].reshape(4, TOK, DK)
        dk_out[span] = both[:, DK:].reshape(4, TOK, DK)
    wait_all(GG)
    for b in range(NBLK):
        both, span = recvs[GG, pl.ds(b * BLK, BLK)].astype(F32), pl.ds(b * 4, 4)
        gf_out[span] = both[:, :DK].reshape(4, TOK, DK)
        gb_out[span] = both[:, DK:].reshape(4, TOK, DK)
    wait_all(GW)
    total = jnp.zeros((TOK, DV), F32)
    for b in range(SP):
        total = total + recvs[GW, pl.ds(b * TOK, TOK)].astype(F32)
    gw_out[...] = total
    for cc in range(4):
        to_core(far * 2 + 1 - core, cc, 3).wait_recv()
        at = pl.ds(pl.multiple_of(((z + 4 - cc) % 4) * BLK, BLK), BLK)
        gh_out[at] = (acc[pl.ds(cc * BLK, BLK)] + term(far, cc)).astype(BF16)

    def left_here(r, carry):
        for kind in range(8):
            sp_copy(kind, r, peer_of(r)).wait_send()
        return carry

    lax.fori_loop(1, SP, left_here, 0)

    def w_left(r, carry):
        w_copy(r).wait_send()
        return carry

    lax.fori_loop(1, TP, w_left, 0)
    for cc in range(4):
        for slot in range(3):
            to_chip(tp, cc, slot, right).wait_send()
        for slot in range(4):
            to_core(tp, cc, slot).wait_send()


def finish(*refs):
    out_sem = refs[-1]
    copies = [pltpu.make_async_copy(refs[i], refs[i + 6], out_sem.at[i]) for i in (2, 3, 0, 1, 4, 5)]
    for copy in copies:
        copy.start()
    for copy in copies:
        copy.wait()


def per_device(hidden, value_weight, queries, key_vectors, forward_decay, backward_decay, cotangent):
    in_hbm = pl.BlockSpec(memory_space=pltpu.HBM)
    vmem = pl.BlockSpec(memory_space=pltpu.VMEM)
    narrow = (BATCH, TOK, DK)
    wide = (ROWS, DV)
    sem = pltpu.SemaphoreType.DMA
    shape = jax.ShapeDtypeStruct
    rows_of = pl.pallas_call(
        kernel,
        out_shape=(
            shape(narrow, BF16),
            shape(narrow, BF16),
            shape(narrow, F32),
            shape(narrow, F32),
            shape(wide, BF16),
            shape((WIDTH // SP, DV), F32),
        ),
        in_specs=[in_hbm] * 7,
        out_specs=(vmem,) * 6,
        scratch_shapes=[
            pltpu.VMEM((BATCH, TOK, WIDTH), BF16),
            pltpu.VMEM((WIDTH, DV), BF16),
            pltpu.VMEM(narrow, BF16),
            pltpu.VMEM(narrow, BF16),
            pltpu.VMEM(narrow, F32),
            pltpu.VMEM(narrow, F32),
            pltpu.VMEM((8, ROWS, DV), BF16),
            pltpu.VMEM((8, ROWS, DV), BF16),
            pltpu.VMEM(wide, BF16),
            pltpu.VMEM(wide, BF16),
            pltpu.VMEM(wide, F32),
            pltpu.VMEM(wide, F32),
            pltpu.VMEM((ROWS, BLK), BF16),
            pltpu.VMEM((2, NBLK * DV, DV), BF16),
            pltpu.VMEM((TP * ROWS, DV), BF16),
            pltpu.VMEM((TP * DV, DV), BF16),
            pltpu.VMEM(wide, F32),
            pltpu.VMEM((WIDTH, ROWS), BF16),
            sem((7,)),
            sem((8, SP)),
            sem((8, SP)),
            sem((8,)),
            sem((TP,)),
            sem((TP,)),
            sem((3, 4)),
            sem((3, 4)),
            sem((4, 4)),
            sem((4, 4)),
        ],
        compiler_params=pltpu.CompilerParams(
            collective_id=0, has_side_effects=True, vmem_limit_bytes=26 << 20
        ),
    )(
        *(
            pltpu.with_memory_space_constraint(operand, pltpu.HBM)
            for operand in (
                hidden,
                value_weight,
                queries.reshape(narrow),
                key_vectors.reshape(narrow),
                forward_decay.reshape(narrow),
                backward_decay.reshape(narrow),
                cotangent.reshape(wide),
            )
        )
    )
    outs = pl.pallas_call(
        finish,
        out_shape=(
            shape(narrow, BF16),
            shape(narrow, BF16),
            shape(narrow, F32),
            shape(narrow, F32),
            shape(wide, BF16),
            shape((WIDTH // SP, DV), F32),
        ),
        in_specs=[vmem] * 6,
        out_specs=(in_hbm,) * 6,
        scratch_shapes=[sem((6,))],
        compiler_params=pltpu.CompilerParams(vmem_limit_bytes=16 << 20),
    )(*rows_of)
    heads = (BATCH, 1, TOK, DK)
    return tuple(out.reshape(heads) for out in outs[:4]) + (outs[4].reshape(BATCH, TOK, DV), outs[5])


def solution(mesh):
    spread = P(None, "tp", "sp", None)
    return jax.shard_map(
        per_device,
        mesh=mesh,
        in_specs=(
            P(None, "sp", None),
            P(None, "tp"),
            spread,
            spread,
            spread,
            spread,
            P(None, "sp", "tp"),
        ),
        out_specs=(spread, spread, spread, spread, P(None, "sp", "tp"), P("sp", "tp")),
        check_vma=False,
    )
```

```python
import functools

import jax
import jax.numpy as jnp
from jax import lax
from jax.experimental import pallas as pl
from jax.experimental.pallas import tpu as pltpu
from jax.sharding import PartitionSpec as P

MESH = pl.DeviceIdType.MESH
F32, BF16 = jnp.float32, jnp.bfloat16
SP, TP = 16, 8
BATCH, TOK, DK, DV, WIDTH = 16, 64, 64, 128, 1024
ROWS = BATCH * TOK
BLK = 256
NBLK = ROWS // BLK
FAR_FIRST = (10, 6, 9, 14, 11, 5, 15, 13, 7, 2, 8, 1, 4, 3, 12)
NEAR_FIRST = FAR_FIRST[::-1]
STEP = 2.0**-16
QK, DEC, DO, VV, DVT, DQK, GG, GW = range(8)


def iota(shape, axis):
    return lax.broadcasted_iota(jnp.int32, shape, axis)


def dot(a, b):
    return lax.dot_general(a, b, (((1,), (0,)), ((), ())), preferred_element_type=F32)


def dot_nt(a, b):
    return lax.dot_general(a, b, (((1,), (1,)), ((), ())), preferred_element_type=F32)


def dot_tn(a, b):
    return lax.dot_general(a, b, (((0,), (0,)), ((), ())), preferred_element_type=F32)


def hi_lo(x):
    hi = x.astype(BF16)
    lo = (x - hi.astype(F32)).astype(BF16)
    return jnp.concatenate([hi, lo], axis=1)


def tri(group):
    r, c = iota((BLK, BLK), 0), iota((BLK, BLK), 1)
    keep = r >= c
    if group < BLK:
        keep = keep & (r // group == c // group)
    return jnp.where(keep, 1.0, 0.0).astype(BF16)


def tile(ref, index):
    return ref.at[pl.ds(pl.multiple_of(index * TOK, TOK), TOK)]


def kernel(
    hidden,
    weight,
    q_hbm,
    k_hbm,
    df_hbm,
    db_hbm,
    cot,
    dq_out,
    dk_out,
    gf_out,
    gb_out,
    gh_out,
    gw_out,
    hid,
    w,
    q_in,
    k_in,
    df_in,
    db_in,
    sends,
    recvs,
    qhat,
    khat,
    grow,
    gterm,
    scores,
    parts,
    dall,
    wx,
    acc,
    hid_t,
    in_sem,
    ss,
    rs,
    loc_sem,
    wss,
    wrs,
    xss,
    xrs,
    pss,
    prs,
):
    me = lax.axis_index("sp")
    tp = lax.axis_index("tp")
    y, z = me % 4, me // 4
    core, xc = tp % 2, tp // 2
    barrier = pltpu.get_barrier_semaphore()

    def greet_sp(r, carry):
        pl.semaphore_signal(
            barrier, inc=1, device_id={"sp": (me + r) % SP}, device_id_type=MESH
        )
        return carry

    def greet_tp(r, carry):
        pl.semaphore_signal(
            barrier, inc=1, device_id={"tp": (tp + r) % TP}, device_id_type=MESH
        )
        return carry

    lax.fori_loop(1, SP, greet_sp, 0)
    lax.fori_loop(1, TP, greet_tp, 0)

    loads = [
        pltpu.make_async_copy(df_hbm, df_in, in_sem.at[2]),
        pltpu.make_async_copy(db_hbm, db_in, in_sem.at[3]),
        pltpu.make_async_copy(q_hbm, q_in, in_sem.at[0]),
        pltpu.make_async_copy(k_hbm, k_in, in_sem.at[1]),
        pltpu.make_async_copy(cot, sends.at[DO], in_sem.at[4]),
        pltpu.make_async_copy(weight, w, in_sem.at[5]),
        pltpu.make_async_copy(hidden, hid, in_sem.at[6]),
    ]
    for load in loads:
        load.start()

    def peer_of(r):
        m = r
        return ((z + m // 4) % 4) * 4 + (y + m % 4) % 4

    def landing(kind, frm):
        if kind == DVT:
            return dall.at[pl.ds(pl.multiple_of(tp * ROWS + frm * TOK, TOK), TOK)]
        return tile(recvs.at[kind], frm)

    def sp_copy(kind, r, to):
        return pltpu.make_async_remote_copy(
            src_ref=tile(sends.at[kind], to),
            dst_ref=landing(kind, me),
            send_sem=ss.at[kind, r],
            recv_sem=rs.at[kind, me],
            device_id={"sp": to},
            device_id_type=MESH,
        )

    def sp_wait(kind, r, frm):
        pltpu.make_async_remote_copy(
            src_ref=landing(kind, frm),
            dst_ref=landing(kind, frm),
            send_sem=ss.at[kind, r],
            recv_sem=rs.at[kind, frm],
            device_id={"sp": frm},
            device_id_type=MESH,
        ).wait_recv()

    def own_copy(kind):
        return pltpu.make_async_copy(
            tile(sends.at[kind], me), landing(kind, me), loc_sem.at[kind]
        )

    def send_all(kind):
        for m in NEAR_FIRST if kind == VV else FAR_FIRST:
            sp_copy(kind, m, peer_of(m)).start()
        own_copy(kind).start()

    def wait_all(kind):
        def body(r, carry):
            sp_wait(kind, r, peer_of(r))
            return carry

        lax.fori_loop(1, SP, body, 0)
        own_copy(kind).wait()

    def send_block(kind, jj, blk):
        for i in range(4):
            if jj == 0 and i == 0:
                own_copy(kind).start()
            else:
                sp_copy(kind, jj * 4 + i, blk * 4 + (y + i) % 4).start()

    def wait_plane(kind, jj, plane):
        for i in range(4):
            if jj == 0 and i == 0:
                own_copy(kind).wait()
            else:
                sp_wait(kind, jj * 4 + i, plane * 4 + (y + i) % 4)

    loads[0].wait()
    loads[1].wait()
    low = tri(TOK)
    for b in range(NBLK):
        span = pl.ds(b * 4, 4)
        both = jnp.concatenate(
            [df_in[span].reshape(BLK, DK), db_in[span].reshape(BLK, DK)], axis=1
        )
        run = dot(low, hi_lo(both))
        steps = jnp.round((run[:, :DV] + run[:, DV:]) * (1.0 / STEP))
        before = jnp.where(iota((BLK, DV), 0) % TOK == 0, 0.0, pltpu.roll(steps, 1, 0))
        sends[DEC, pl.ds(b * BLK, BLK)] = ((steps - before) * STEP).astype(BF16)
    loads[2].wait()
    loads[3].wait()
    sends[QK] = jnp.concatenate(
        [q_in[...].reshape(ROWS, DK), k_in[...].reshape(ROWS, DK)], axis=1
    )
    loads[4].wait()
    loads[5].wait()
    pl.semaphore_wait(barrier, SP + TP - 2)
    send_all(DEC)
    send_all(QK)
    send_all(DO)

    def w_copy(r):
        to = (tp + r) % TP
        return pltpu.make_async_remote_copy(
            src_ref=w.at[pl.ds(pl.multiple_of(to * DV, DV), DV)],
            dst_ref=wx.at[pl.ds(pl.multiple_of(tp * DV, DV), DV)],
            send_sem=wss.at[r],
            recv_sem=wrs.at[r],
            device_id={"tp": to},
            device_id_type=MESH,
        )

    def w_send(r, carry):
        w_copy(r).start()
        return carry

    lax.fori_loop(1, TP, w_send, 0)
    own_w = pltpu.make_async_copy(
        w.at[pl.ds(pl.multiple_of(tp * DV, DV), DV)],
        wx.at[pl.ds(pl.multiple_of(tp * DV, DV), DV)],
        wrs.at[0],
    )
    own_w.start()

    loads[6].wait()
    for b in range(NBLK):
        rows = hid[pl.ds(b * 4, 4)].reshape(BLK, WIDTH)
        sends[VV, pl.ds(b * BLK, BLK)] = dot(rows, w[...]).astype(BF16)
    send_all(VV)

    def turn(t, carry):
        at = pl.ds(pl.multiple_of(t * 128, 128), 128)
        hid_t[:, at] = hid[pl.ds(t * 2, 2)].reshape(128, WIDTH).T
        return carry

    lax.fori_loop(0, ROWS // 128, turn, 0)

    wait_all(DEC)
    lane_f = iota((BLK, DV), 1) < DK
    full = tri(BLK)
    base = jnp.zeros((1, DV), F32)
    cums = []
    for b in range(NBLK):
        d = recvs[DEC, pl.ds(b * BLK, BLK)]
        inside = dot(full, d) + base
        base = inside[BLK - 1 :, :]
        cums.append(jnp.where(lane_f, inside, d.astype(F32) - inside))
    wait_all(QK)
    r_, c_ = iota((BLK, BLK), 0), iota((BLK, BLK), 1)
    zero16 = jnp.zeros((), BF16)
    for b in range(NBLK):
        at = pl.ds(b * BLK, BLK)
        growth = jnp.exp(cums[b])
        shrink = jnp.exp(-cums[b])
        qk = recvs[QK, at].astype(F32)
        kq = pltpu.roll(qk, DK, 1)
        qh = (jnp.where(lane_f, qk, kq) * growth).astype(BF16)
        kh = (jnp.where(lane_f, kq, qk) * shrink).astype(BF16)
        qhat[at] = qh
        khat[at] = kh
        grow[at] = growth
        fwd = dot_nt(jnp.where(lane_f, kh, zero16), qh)
        bwd = dot_nt(jnp.where(lane_f, zero16, kh), qh)
        both = jnp.where(r_ <= c_, fwd, 0.0) + jnp.where(r_ >= c_, bwd, 0.0)
        scores[at] = both.astype(BF16)
    row_f = iota((DV, DV), 0) < DK

    def others(pieces):
        zero = jnp.zeros((DV, DV), F32)
        after, before = [zero] * NBLK, [zero] * NBLK
        for b in range(NBLK - 2, -1, -1):
            after[b] = after[b + 1] + pieces[b + 1]
        for b in range(1, NBLK):
            before[b] = before[b - 1] + pieces[b - 1]
        return after, before

    wait_all(DO)
    pieces = [
        dot_tn(qhat[pl.ds(b * BLK, BLK)], recvs[DO, pl.ds(b * BLK, BLK)]) for b in range(NBLK)
    ]
    after, before = others(pieces)
    for b in range(NBLK):
        parts[0, pl.ds(b * DV, DV)] = jnp.where(row_f, after[b], before[b]).astype(BF16)
    for jj in range(NBLK):
        blk = (z + jj) % NBLK
        at = pl.ds(pl.multiple_of(blk * BLK, BLK), BLK)
        pat = pl.ds(pl.multiple_of(blk * DV, DV), DV)
        dv = dot(khat[at], parts[0, pat]) + dot(scores[at], recvs[DO, at])
        sends[DVT, at] = dv.astype(BF16)
        send_block(DVT, jj, blk)

    right, left, far = (xc + 1) % 4, (xc + 3) % 4, (xc + 2) % 4

    def piece(head, cc):
        row = head * ROWS + ((z + 4 - cc) % 4) * BLK
        return dall.at[pl.ds(pl.multiple_of(row, BLK), BLK)]

    def hop(head, cc, sems_s, sems_r, slot, to):
        return pltpu.make_async_remote_copy(
            src_ref=piece(head, cc),
            dst_ref=piece(head, cc),
            send_sem=sems_s.at[slot, cc],
            recv_sem=sems_r.at[slot, cc],
            device_id={"tp": to},
            device_id_type=MESH,
        )

    def to_chip(head, cc, slot, chip):
        return hop(head, cc, xss, xrs, slot, chip * 2 + core)

    def to_core(head, cc, slot):
        return hop(head, cc, pss, prs, slot, xc * 2 + 1 - core)

    def first_hops(cc):
        wait_plane(DVT, cc, (z + 4 - cc) % 4)
        to_chip(tp, cc, 0, right).start()
        to_chip(tp, cc, 1, left).start()
        to_core(tp, cc, 0).start()

    wait_all(VV)
    pieces = [
        dot_tn(khat[pl.ds(b * BLK, BLK)], recvs[VV, pl.ds(b * BLK, BLK)]) for b in range(NBLK)
    ]
    after, before = others(pieces)
    for b in range(NBLK):
        parts[1, pl.ds(b * DV, DV)] = jnp.where(row_f, before[b], after[b]).astype(BF16)
    for jj in range(NBLK):
        blk = (z + jj) % NBLK
        at = pl.ds(pl.multiple_of(blk * BLK, BLK), BLK)
        pat = pl.ds(pl.multiple_of(blk * DV, DV), DV)
        qh, kh, do, v = qhat[at], khat[at], recvs[DO, at], recvs[VV, at]
        growth = grow[at]
        s = dot_nt(do, v).astype(BF16)
        st = dot_nt(v, do).astype(BF16)
        x = dot_nt(do, parts[1, pat])
        x = x + dot(jnp.where(r_ >= c_, s, zero16), jnp.where(lane_f, kh, zero16))
        x = x + dot(jnp.where(r_ <= c_, s, zero16), jnp.where(lane_f, zero16, kh))
        yk = dot_nt(v, parts[0, pat])
        yk = yk + dot(jnp.where(r_ <= c_, st, zero16), jnp.where(lane_f, qh, zero16))
        yk = yk + dot(jnp.where(r_ >= c_, st, zero16), jnp.where(lane_f, zero16, qh))
        gterm[at] = qh.astype(F32) * x - kh.astype(F32) * yk
        dq2 = x * growth
        dk2 = yk / growth
        dq2 = dq2 + pltpu.roll(dq2, DK, 1)
        dk2 = dk2 + pltpu.roll(dk2, DK, 1)
        sends[DQK, at] = jnp.where(lane_f, dq2, dk2).astype(BF16)
        send_block(DQK, jj, blk)
        first_hops(jj)
    base = jnp.zeros((1, DV), F32)
    for b in range(NBLK):
        at = pl.ds(b * BLK, BLK)
        g = gterm[at]
        run = dot(full, hi_lo(g))
        run = run[:, :DV] + run[:, DV:] + base
        base = run[BLK - 1 :, :]
        sends[GG, at] = jnp.where(lane_f, g - run, run).astype(BF16)

    drows = dall[pl.ds(pl.multiple_of(tp * ROWS, ROWS), ROWS)]
    for b in range(NBLK):
        at = pl.ds(b * BLK, BLK)
        sends[GW, at] = dot(hid_t[at], drows).astype(BF16)
    send_all(GW)
    send_all(GG)

    def w_arrived(r, carry):
        frm = (tp + TP - r) % TP
        spot = wx.at[pl.ds(pl.multiple_of(frm * DV, DV), DV)]
        pltpu.make_async_remote_copy(
            src_ref=spot,
            dst_ref=spot,
            send_sem=wss.at[r],
            recv_sem=wrs.at[r],
            device_id={"tp": frm},
            device_id_type=MESH,
        ).wait_recv()
        return carry

    lax.fori_loop(1, TP, w_arrived, 0)
    own_w.wait()

    def term(chip, cc):
        total = None
        for c in range(2):
            head = chip * 2 + c
            row = head * ROWS + ((z + 4 - cc) % 4) * BLK
            rows = dall[pl.ds(pl.multiple_of(row, BLK), BLK)]
            part = dot_nt(rows, wx[pl.ds(pl.multiple_of(head * DV, DV), DV)])
            total = part if total is None else total + part
        return total

    for cc in range(4):
        head_l, head_r = left * 2 + core, right * 2 + core
        to_chip(head_l, cc, 0, left).wait_recv()
        if cc % 2 == 0:
            to_chip(head_l, cc, 2, right).start()
        to_core(head_l, cc, 1).start()
        to_chip(head_r, cc, 1, right).wait_recv()
        if cc % 2 == 1:
            to_chip(head_r, cc, 2, left).start()
        to_core(head_r, cc, 2).start()
    for cc in range(4):
        for slot, chip in ((0, xc), (1, left), (2, right)):
            to_core(chip * 2 + 1 - core, cc, slot).wait_recv()
        acc[pl.ds(cc * BLK, BLK)] = term(xc, cc) + term(left, cc) + term(right, cc)
    for cc in range(4):
        to_chip(far * 2 + core, cc, 2, far).wait_recv()
        to_core(far * 2 + core, cc, 3).start()

    wait_all(DQK)
    for b in range(NBLK):
        both, span = recvs[DQK, pl.ds(b * BLK, BLK)], pl.ds(b * 4, 4)
        dq_out[span] = both[:, :DK].reshape(4, TOK, DK)
        dk_out[span] = both[:, DK:].reshape(4, TOK, DK)
    wait_all(GG)
    for b in range(NBLK):
        both, span = recvs[GG, pl.ds(b * BLK, BLK)].astype(F32), pl.ds(b * 4, 4)
        gf_out[span] = both[:, :DK].reshape(4, TOK, DK)
        gb_out[span] = both[:, DK:].reshape(4, TOK, DK)
    wait_all(GW)
    total = jnp.zeros((TOK, DV), F32)
    for b in range(SP):
        total = total + recvs[GW, pl.ds(b * TOK, TOK)].astype(F32)
    gw_out[...] = total
    for cc in range(4):
        to_core(far * 2 + 1 - core, cc, 3).wait_recv()
        at = pl.ds(pl.multiple_of(((z + 4 - cc) % 4) * BLK, BLK), BLK)
        gh_out[at] = (acc[pl.ds(cc * BLK, BLK)] + term(far, cc)).astype(BF16)

    def left_here(r, carry):
        for kind in range(8):
            sp_copy(kind, r, peer_of(r)).wait_send()
        return carry

    lax.fori_loop(1, SP, left_here, 0)

    def w_left(r, carry):
        w_copy(r).wait_send()
        return carry

    lax.fori_loop(1, TP, w_left, 0)
    for cc in range(4):
        for slot in range(3):
            to_chip(tp, cc, slot, right).wait_send()
        for slot in range(4):
            to_core(tp, cc, slot).wait_send()


def finish(*refs):
    out_sem = refs[-1]
    copies = [pltpu.make_async_copy(refs[i], refs[i + 6], out_sem.at[i]) for i in (2, 3, 0, 1, 4, 5)]
    for copy in copies:
        copy.start()
    for copy in copies:
        copy.wait()


def per_device(hidden, value_weight, queries, key_vectors, forward_decay, backward_decay, cotangent):
    in_hbm = pl.BlockSpec(memory_space=pltpu.HBM)
    vmem = pl.BlockSpec(memory_space=pltpu.VMEM)
    narrow = (BATCH, TOK, DK)
    wide = (ROWS, DV)
    sem = pltpu.SemaphoreType.DMA
    shape = jax.ShapeDtypeStruct
    rows_of = pl.pallas_call(
        kernel,
        out_shape=(
            shape(narrow, BF16),
            shape(narrow, BF16),
            shape(narrow, F32),
            shape(narrow, F32),
            shape(wide, BF16),
            shape((WIDTH // SP, DV), F32),
        ),
        in_specs=[in_hbm] * 7,
        out_specs=(vmem,) * 6,
        scratch_shapes=[
            pltpu.VMEM((BATCH, TOK, WIDTH), BF16),
            pltpu.VMEM((WIDTH, DV), BF16),
            pltpu.VMEM(narrow, BF16),
            pltpu.VMEM(narrow, BF16),
            pltpu.VMEM(narrow, F32),
            pltpu.VMEM(narrow, F32),
            pltpu.VMEM((8, ROWS, DV), BF16),
            pltpu.VMEM((8, ROWS, DV), BF16),
            pltpu.VMEM(wide, BF16),
            pltpu.VMEM(wide, BF16),
            pltpu.VMEM(wide, F32),
            pltpu.VMEM(wide, F32),
            pltpu.VMEM((ROWS, BLK), BF16),
            pltpu.VMEM((2, NBLK * DV, DV), BF16),
            pltpu.VMEM((TP * ROWS, DV), BF16),
            pltpu.VMEM((TP * DV, DV), BF16),
            pltpu.VMEM(wide, F32),
            pltpu.VMEM((WIDTH, ROWS), BF16),
            sem((7,)),
            sem((8, SP)),
            sem((8, SP)),
            sem((8,)),
            sem((TP,)),
            sem((TP,)),
            sem((3, 4)),
            sem((3, 4)),
            sem((4, 4)),
            sem((4, 4)),
        ],
        compiler_params=pltpu.CompilerParams(
            collective_id=0, has_side_effects=True, vmem_limit_bytes=26 << 20
        ),
    )(
        *(
            pltpu.with_memory_space_constraint(operand, pltpu.HBM)
            for operand in (
                hidden,
                value_weight,
                queries.reshape(narrow),
                key_vectors.reshape(narrow),
                forward_decay.reshape(narrow),
                backward_decay.reshape(narrow),
                cotangent.reshape(wide),
            )
        )
    )
    outs = pl.pallas_call(
        finish,
        out_shape=(
            shape(narrow, BF16),
            shape(narrow, BF16),
            shape(narrow, F32),
            shape(narrow, F32),
            shape(wide, BF16),
            shape((WIDTH // SP, DV), F32),
        ),
        in_specs=[vmem] * 6,
        out_specs=(in_hbm,) * 6,
        scratch_shapes=[sem((6,))],
        compiler_params=pltpu.CompilerParams(vmem_limit_bytes=16 << 20),
    )(*rows_of)
    heads = (BATCH, 1, TOK, DK)
    return tuple(out.reshape(heads) for out in outs[:4]) + (outs[4].reshape(BATCH, TOK, DV), outs[5])


def solution(mesh):
    spread = P(None, "tp", "sp", None)
    return jax.shard_map(
        per_device,
        mesh=mesh,
        in_specs=(
            P(None, "sp", None),
            P(None, "tp"),
            spread,
            spread,
            spread,
            spread,
            P(None, "sp", "tp"),
        ),
        out_specs=(spread, spread, spread, spread, P(None, "sp", "tp"), P("sp", "tp")),
        check_vma=False,
    )
```

```python
import functools

import jax
import jax.numpy as jnp
from jax import lax
from jax.experimental import pallas as pl
from jax.experimental.pallas import tpu as pltpu
from jax.sharding import PartitionSpec as P

MESH = pl.DeviceIdType.MESH
F32, BF16 = jnp.float32, jnp.bfloat16
SP, TP = 16, 8
BATCH, TOK, DK, DV, WIDTH = 16, 64, 64, 128, 1024
ROWS = BATCH * TOK
BLK = 256
NBLK = ROWS // BLK
FAR_FIRST = (10, 6, 9, 14, 11, 5, 15, 13, 7, 2, 8, 1, 4, 3, 12)
NEAR_FIRST = FAR_FIRST[::-1]
STEP = 2.0**-16
QK, DEC, DO, VV, DVT, DQK, GG, GW = range(8)


def iota(shape, axis):
    return lax.broadcasted_iota(jnp.int32, shape, axis)


def dot(a, b):
    return lax.dot_general(a, b, (((1,), (0,)), ((), ())), preferred_element_type=F32)


def dot_nt(a, b):
    return lax.dot_general(a, b, (((1,), (1,)), ((), ())), preferred_element_type=F32)


def dot_tn(a, b):
    return lax.dot_general(a, b, (((0,), (0,)), ((), ())), preferred_element_type=F32)


def hi_lo(x):
    hi = x.astype(BF16)
    lo = (x - hi.astype(F32)).astype(BF16)
    return jnp.concatenate([hi, lo], axis=1)


def tri(group):
    r, c = iota((BLK, BLK), 0), iota((BLK, BLK), 1)
    keep = r >= c
    if group < BLK:
        keep = keep & (r // group == c // group)
    return jnp.where(keep, 1.0, 0.0).astype(BF16)


def tile(ref, index):
    return ref.at[pl.ds(pl.multiple_of(index * TOK, TOK), TOK)]


def kernel(
    hidden,
    weight,
    q_hbm,
    k_hbm,
    df_hbm,
    db_hbm,
    cot,
    dq_out,
    dk_out,
    gf_out,
    gb_out,
    gh_out,
    gw_out,
    hid,
    w,
    q_in,
    k_in,
    df_in,
    db_in,
    sends,
    recvs,
    qhat,
    khat,
    grow,
    gterm,
    scores,
    parts,
    dall,
    wx,
    acc,
    hid_t,
    in_sem,
    ss,
    rs,
    loc_sem,
    wss,
    wrs,
    xss,
    xrs,
    pss,
    prs,
):
    me = lax.axis_index("sp")
    tp = lax.axis_index("tp")
    y, z = me % 4, me // 4
    core, xc = tp % 2, tp // 2
    barrier = pltpu.get_barrier_semaphore()

    def greet_sp(r, carry):
        pl.semaphore_signal(
            barrier, inc=1, device_id={"sp": (me + r) % SP}, device_id_type=MESH
        )
        return carry

    def greet_tp(r, carry):
        pl.semaphore_signal(
            barrier, inc=1, device_id={"tp": (tp + r) % TP}, device_id_type=MESH
        )
        return carry

    lax.fori_loop(1, SP, greet_sp, 0)
    lax.fori_loop(1, TP, greet_tp, 0)

    loads = [
        pltpu.make_async_copy(df_hbm, df_in, in_sem.at[2]),
        pltpu.make_async_copy(db_hbm, db_in, in_sem.at[3]),
        pltpu.make_async_copy(q_hbm, q_in, in_sem.at[0]),
        pltpu.make_async_copy(k_hbm, k_in, in_sem.at[1]),
        pltpu.make_async_copy(cot, sends.at[DO], in_sem.at[4]),
        pltpu.make_async_copy(weight, w, in_sem.at[5]),
        pltpu.make_async_copy(hidden, hid, in_sem.at[6]),
    ]
    for load in loads:
        load.start()

    def peer_of(r):
        m = r
        return ((z + m // 4) % 4) * 4 + (y + m % 4) % 4

    def landing(kind, frm):
        if kind == DVT:
            return dall.at[pl.ds(pl.multiple_of(tp * ROWS + frm * TOK, TOK), TOK)]
        return tile(recvs.at[kind], frm)

    def sp_copy(kind, r, to):
        return pltpu.make_async_remote_copy(
            src_ref=tile(sends.at[kind], to),
            dst_ref=landing(kind, me),
            send_sem=ss.at[kind, r],
            recv_sem=rs.at[kind, me],
            device_id={"sp": to},
            device_id_type=MESH,
        )

    def sp_wait(kind, r, frm):
        pltpu.make_async_remote_copy(
            src_ref=landing(kind, frm),
            dst_ref=landing(kind, frm),
            send_sem=ss.at[kind, r],
            recv_sem=rs.at[kind, frm],
            device_id={"sp": frm},
            device_id_type=MESH,
        ).wait_recv()

    def own_copy(kind):
        return pltpu.make_async_copy(
            tile(sends.at[kind], me), landing(kind, me), loc_sem.at[kind]
        )

    def send_all(kind):
        for m in NEAR_FIRST if kind == VV else FAR_FIRST:
            sp_copy(kind, m, peer_of(m)).start()
        own_copy(kind).start()

    def wait_all(kind):
        def body(r, carry):
            sp_wait(kind, r, peer_of(r))
            return carry

        lax.fori_loop(1, SP, body, 0)
        own_copy(kind).wait()

    def send_block(kind, jj, blk):
        for i in range(4):
            if jj == 0 and i == 0:
                own_copy(kind).start()
            else:
                sp_copy(kind, jj * 4 + i, blk * 4 + (y + i) % 4).start()

    def wait_plane(kind, jj, plane):
        for i in range(4):
            if jj == 0 and i == 0:
                own_copy(kind).wait()
            else:
                sp_wait(kind, jj * 4 + i, plane * 4 + (y + i) % 4)

    loads[0].wait()
    loads[1].wait()
    low = tri(TOK)
    for b in range(NBLK):
        span = pl.ds(b * 4, 4)
        both = jnp.concatenate(
            [df_in[span].reshape(BLK, DK), db_in[span].reshape(BLK, DK)], axis=1
        )
        run = dot(low, hi_lo(both))
        steps = jnp.round((run[:, :DV] + run[:, DV:]) * (1.0 / STEP))
        before = jnp.where(iota((BLK, DV), 0) % TOK == 0, 0.0, pltpu.roll(steps, 1, 0))
        sends[DEC, pl.ds(b * BLK, BLK)] = ((steps - before) * STEP).astype(BF16)
    loads[2].wait()
    loads[3].wait()
    sends[QK] = jnp.concatenate(
        [q_in[...].reshape(ROWS, DK), k_in[...].reshape(ROWS, DK)], axis=1
    )
    loads[4].wait()
    loads[5].wait()
    pl.semaphore_wait(barrier, SP + TP - 2)
    send_all(DEC)
    send_all(QK)
    send_all(DO)

    def w_copy(r):
        to = (tp + r) % TP
        return pltpu.make_async_remote_copy(
            src_ref=w.at[pl.ds(pl.multiple_of(to * DV, DV), DV)],
            dst_ref=wx.at[pl.ds(pl.multiple_of(tp * DV, DV), DV)],
            send_sem=wss.at[r],
            recv_sem=wrs.at[r],
            device_id={"tp": to},
            device_id_type=MESH,
        )

    def w_send(r, carry):
        w_copy(r).start()
        return carry

    lax.fori_loop(1, TP, w_send, 0)
    own_w = pltpu.make_async_copy(
        w.at[pl.ds(pl.multiple_of(tp * DV, DV), DV)],
        wx.at[pl.ds(pl.multiple_of(tp * DV, DV), DV)],
        wrs.at[0],
    )
    own_w.start()

    loads[6].wait()
    for b in range(NBLK):
        rows = hid[pl.ds(b * 4, 4)].reshape(BLK, WIDTH)
        sends[VV, pl.ds(b * BLK, BLK)] = dot(rows, w[...]).astype(BF16)
    send_all(VV)

    def turn(t, carry):
        at = pl.ds(pl.multiple_of(t * 128, 128), 128)
        hid_t[:, at] = hid[pl.ds(t * 2, 2)].reshape(128, WIDTH).T
        return carry

    lax.fori_loop(0, ROWS // 128, turn, 0)

    wait_all(DEC)
    lane_f = iota((BLK, DV), 1) < DK
    full = tri(BLK)
    base = jnp.zeros((1, DV), F32)
    cums = []
    for b in range(NBLK):
        d = recvs[DEC, pl.ds(b * BLK, BLK)]
        inside = dot(full, d) + base
        base = inside[BLK - 1 :, :]
        cums.append(jnp.where(lane_f, inside, d.astype(F32) - inside))
    wait_all(QK)
    r_, c_ = iota((BLK, BLK), 0), iota((BLK, BLK), 1)
    zero16 = jnp.zeros((), BF16)
    for b in range(NBLK):
        at = pl.ds(b * BLK, BLK)
        growth = jnp.exp(cums[b])
        shrink = jnp.exp(-cums[b])
        qk = recvs[QK, at].astype(F32)
        kq = pltpu.roll(qk, DK, 1)
        qh = (jnp.where(lane_f, qk, kq) * growth).astype(BF16)
        kh = (jnp.where(lane_f, kq, qk) * shrink).astype(BF16)
        qhat[at] = qh
        khat[at] = kh
        grow[at] = growth
        fwd = dot_nt(jnp.where(lane_f, kh, zero16), qh)
        bwd = dot_nt(jnp.where(lane_f, zero16, kh), qh)
        both = jnp.where(r_ <= c_, fwd, 0.0) + jnp.where(r_ >= c_, bwd, 0.0)
        scores[at] = both.astype(BF16)
    row_f = iota((DV, DV), 0) < DK

    def others(pieces):
        zero = jnp.zeros((DV, DV), F32)
        after, before = [zero] * NBLK, [zero] * NBLK
        for b in range(NBLK - 2, -1, -1):
            after[b] = after[b + 1] + pieces[b + 1]
        for b in range(1, NBLK):
            before[b] = before[b - 1] + pieces[b - 1]
        return after, before

    wait_all(DO)
    pieces = [
        dot_tn(qhat[pl.ds(b * BLK, BLK)], recvs[DO, pl.ds(b * BLK, BLK)]) for b in range(NBLK)
    ]
    after, before = others(pieces)
    for b in range(NBLK):
        parts[0, pl.ds(b * DV, DV)] = jnp.where(row_f, after[b], before[b]).astype(BF16)
    for jj in range(NBLK):
        blk = (z + jj) % NBLK
        at = pl.ds(pl.multiple_of(blk * BLK, BLK), BLK)
        pat = pl.ds(pl.multiple_of(blk * DV, DV), DV)
        dv = dot(khat[at], parts[0, pat]) + dot(scores[at], recvs[DO, at])
        sends[DVT, at] = dv.astype(BF16)
        send_block(DVT, jj, blk)

    right, left, far = (xc + 1) % 4, (xc + 3) % 4, (xc + 2) % 4

    def piece(head, cc):
        row = head * ROWS + ((z + 4 - cc) % 4) * BLK
        return dall.at[pl.ds(pl.multiple_of(row, BLK), BLK)]

    def hop(head, cc, sems_s, sems_r, slot, to):
        return pltpu.make_async_remote_copy(
            src_ref=piece(head, cc),
            dst_ref=piece(head, cc),
            send_sem=sems_s.at[slot, cc],
            recv_sem=sems_r.at[slot, cc],
            device_id={"tp": to},
            device_id_type=MESH,
        )

    def to_chip(head, cc, slot, chip):
        return hop(head, cc, xss, xrs, slot, chip * 2 + core)

    def to_core(head, cc, slot):
        return hop(head, cc, pss, prs, slot, xc * 2 + 1 - core)

    def first_hops(cc):
        wait_plane(DVT, cc, (z + 4 - cc) % 4)
        to_chip(tp, cc, 0, right).start()
        to_chip(tp, cc, 1, left).start()
        to_core(tp, cc, 0).start()

    wait_all(VV)
    pieces = [
        dot_tn(khat[pl.ds(b * BLK, BLK)], recvs[VV, pl.ds(b * BLK, BLK)]) for b in range(NBLK)
    ]
    after, before = others(pieces)
    for b in range(NBLK):
        parts[1, pl.ds(b * DV, DV)] = jnp.where(row_f, before[b], after[b]).astype(BF16)
    for jj in range(NBLK):
        blk = (z + jj) % NBLK
        at = pl.ds(pl.multiple_of(blk * BLK, BLK), BLK)
        pat = pl.ds(pl.multiple_of(blk * DV, DV), DV)
        qh, kh, do, v = qhat[at], khat[at], recvs[DO, at], recvs[VV, at]
        growth = grow[at]
        s = dot_nt(do, v).astype(BF16)
        st = dot_nt(v, do).astype(BF16)
        x = dot_nt(do, parts[1, pat])
        x = x + dot(jnp.where(r_ >= c_, s, zero16), jnp.where(lane_f, kh, zero16))
        x = x + dot(jnp.where(r_ <= c_, s, zero16), jnp.where(lane_f, zero16, kh))
        yk = dot_nt(v, parts[0, pat])
        yk = yk + dot(jnp.where(r_ <= c_, st, zero16), jnp.where(lane_f, qh, zero16))
        yk = yk + dot(jnp.where(r_ >= c_, st, zero16), jnp.where(lane_f, zero16, qh))
        gterm[at] = qh.astype(F32) * x - kh.astype(F32) * yk
        dq2 = x * growth
        dk2 = yk / growth
        dq2 = dq2 + pltpu.roll(dq2, DK, 1)
        dk2 = dk2 + pltpu.roll(dk2, DK, 1)
        sends[DQK, at] = jnp.where(lane_f, dq2, dk2).astype(BF16)
        send_block(DQK, jj, blk)
        first_hops(jj)
    base = jnp.zeros((1, DV), F32)
    for b in range(NBLK):
        at = pl.ds(b * BLK, BLK)
        g = gterm[at]
        run = dot(full, hi_lo(g))
        run = run[:, :DV] + run[:, DV:] + base
        base = run[BLK - 1 :, :]
        sends[GG, at] = jnp.where(lane_f, g - run, run).astype(BF16)

    drows = dall[pl.ds(pl.multiple_of(tp * ROWS, ROWS), ROWS)]
    for b in range(NBLK):
        at = pl.ds(b * BLK, BLK)
        sends[GW, at] = dot(hid_t[at], drows).astype(BF16)
    send_all(GW)
    send_all(GG)

    def w_arrived(r, carry):
        frm = (tp + TP - r) % TP
        spot = wx.at[pl.ds(pl.multiple_of(frm * DV, DV), DV)]
        pltpu.make_async_remote_copy(
            src_ref=spot,
            dst_ref=spot,
            send_sem=wss.at[r],
            recv_sem=wrs.at[r],
            device_id={"tp": frm},
            device_id_type=MESH,
        ).wait_recv()
        return carry

    lax.fori_loop(1, TP, w_arrived, 0)
    own_w.wait()

    def term(chip, cc):
        total = None
        for c in range(2):
            head = chip * 2 + c
            row = head * ROWS + ((z + 4 - cc) % 4) * BLK
            rows = dall[pl.ds(pl.multiple_of(row, BLK), BLK)]
            part = dot_nt(rows, wx[pl.ds(pl.multiple_of(head * DV, DV), DV)])
            total = part if total is None else total + part
        return total

    for cc in range(4):
        head_l, head_r = left * 2 + core, right * 2 + core
        to_chip(head_l, cc, 0, left).wait_recv()
        if cc < 2:
            to_chip(head_l, cc, 2, right).start()
        to_core(head_l, cc, 1).start()
        to_chip(head_r, cc, 1, right).wait_recv()
        if cc >= 2:
            to_chip(head_r, cc, 2, left).start()
        to_core(head_r, cc, 2).start()
    for cc in range(4):
        for slot, chip in ((0, xc), (1, left), (2, right)):
            to_core(chip * 2 + 1 - core, cc, slot).wait_recv()
        acc[pl.ds(cc * BLK, BLK)] = term(xc, cc) + term(left, cc) + term(right, cc)
    for cc in range(4):
        to_chip(far * 2 + core, cc, 2, far).wait_recv()
        to_core(far * 2 + core, cc, 3).start()

    wait_all(DQK)
    for b in range(NBLK):
        both, span = recvs[DQK, pl.ds(b * BLK, BLK)], pl.ds(b * 4, 4)
        dq_out[span] = both[:, :DK].reshape(4, TOK, DK)
        dk_out[span] = both[:, DK:].reshape(4, TOK, DK)
    wait_all(GG)
    for b in range(NBLK):
        both, span = recvs[GG, pl.ds(b * BLK, BLK)].astype(F32), pl.ds(b * 4, 4)
        gf_out[span] = both[:, :DK].reshape(4, TOK, DK)
        gb_out[span] = both[:, DK:].reshape(4, TOK, DK)
    wait_all(GW)
    total = jnp.zeros((TOK, DV), F32)
    for b in range(SP):
        total = total + recvs[GW, pl.ds(b * TOK, TOK)].astype(F32)
    gw_out[...] = total
    for cc in range(4):
        to_core(far * 2 + 1 - core, cc, 3).wait_recv()
        at = pl.ds(pl.multiple_of(((z + 4 - cc) % 4) * BLK, BLK), BLK)
        gh_out[at] = (acc[pl.ds(cc * BLK, BLK)] + term(far, cc)).astype(BF16)

    def left_here(r, carry):
        for kind in range(8):
            sp_copy(kind, r, peer_of(r)).wait_send()
        return carry

    lax.fori_loop(1, SP, left_here, 0)

    def w_left(r, carry):
        w_copy(r).wait_send()
        return carry

    lax.fori_loop(1, TP, w_left, 0)
    for cc in range(4):
        for slot in range(3):
            to_chip(tp, cc, slot, right).wait_send()
        for slot in range(4):
            to_core(tp, cc, slot).wait_send()


def finish(*refs):
    out_sem = refs[-1]
    copies = [pltpu.make_async_copy(refs[i], refs[i + 6], out_sem.at[i]) for i in (2, 3, 0, 1, 4, 5)]
    for copy in copies:
        copy.start()
    for copy in copies:
        copy.wait()


def per_device(hidden, value_weight, queries, key_vectors, forward_decay, backward_decay, cotangent):
    in_hbm = pl.BlockSpec(memory_space=pltpu.HBM)
    vmem = pl.BlockSpec(memory_space=pltpu.VMEM)
    narrow = (BATCH, TOK, DK)
    wide = (ROWS, DV)
    sem = pltpu.SemaphoreType.DMA
    shape = jax.ShapeDtypeStruct
    rows_of = pl.pallas_call(
        kernel,
        out_shape=(
            shape(narrow, BF16),
            shape(narrow, BF16),
            shape(narrow, F32),
            shape(narrow, F32),
            shape(wide, BF16),
            shape((WIDTH // SP, DV), F32),
        ),
        in_specs=[in_hbm] * 7,
        out_specs=(vmem,) * 6,
        scratch_shapes=[
            pltpu.VMEM((BATCH, TOK, WIDTH), BF16),
            pltpu.VMEM((WIDTH, DV), BF16),
            pltpu.VMEM(narrow, BF16),
            pltpu.VMEM(narrow, BF16),
            pltpu.VMEM(narrow, F32),
            pltpu.VMEM(narrow, F32),
            pltpu.VMEM((8, ROWS, DV), BF16),
            pltpu.VMEM((8, ROWS, DV), BF16),
            pltpu.VMEM(wide, BF16),
            pltpu.VMEM(wide, BF16),
            pltpu.VMEM(wide, F32),
            pltpu.VMEM(wide, F32),
            pltpu.VMEM((ROWS, BLK), BF16),
            pltpu.VMEM((2, NBLK * DV, DV), BF16),
            pltpu.VMEM((TP * ROWS, DV), BF16),
            pltpu.VMEM((TP * DV, DV), BF16),
            pltpu.VMEM(wide, F32),
            pltpu.VMEM((WIDTH, ROWS), BF16),
            sem((7,)),
            sem((8, SP)),
            sem((8, SP)),
            sem((8,)),
            sem((TP,)),
            sem((TP,)),
            sem((3, 4)),
            sem((3, 4)),
            sem((4, 4)),
            sem((4, 4)),
        ],
        compiler_params=pltpu.CompilerParams(
            collective_id=0, has_side_effects=True, vmem_limit_bytes=26 << 20
        ),
    )(
        *(
            pltpu.with_memory_space_constraint(operand, pltpu.HBM)
            for operand in (
                hidden,
                value_weight,
                queries.reshape(narrow),
                key_vectors.reshape(narrow),
                forward_decay.reshape(narrow),
                backward_decay.reshape(narrow),
                cotangent.reshape(wide),
            )
        )
    )
    outs = pl.pallas_call(
        finish,
        out_shape=(
            shape(narrow, BF16),
            shape(narrow, BF16),
            shape(narrow, F32),
            shape(narrow, F32),
            shape(wide, BF16),
            shape((WIDTH // SP, DV), F32),
        ),
        in_specs=[vmem] * 6,
        out_specs=(in_hbm,) * 6,
        scratch_shapes=[sem((6,))],
        compiler_params=pltpu.CompilerParams(vmem_limit_bytes=16 << 20),
    )(*rows_of)
    heads = (BATCH, 1, TOK, DK)
    return tuple(out.reshape(heads) for out in outs[:4]) + (outs[4].reshape(BATCH, TOK, DV), outs[5])


def solution(mesh):
    spread = P(None, "tp", "sp", None)
    return jax.shard_map(
        per_device,
        mesh=mesh,
        in_specs=(
            P(None, "sp", None),
            P(None, "tp"),
            spread,
            spread,
            spread,
            spread,
            P(None, "sp", "tp"),
        ),
        out_specs=(spread, spread, spread, spread, P(None, "sp", "tp"), P("sp", "tp")),
        check_vma=False,
    )
```
